128 devices in a mesh: sp: 16 (over z, y), dp: 8 (over x, core).
Axes of the slice: x: 4, y: 4, z: 4, core: 2. Of those that a mesh axis runs over, the one named last changes fastest.
Arguments:
- tokens: bfloat16 [8, 8192, 2048], P('dp', 'sp'), may hold values from -6 to 6
- norm_gain: float32 [2048], replicated, may hold values from 0.1 to 1.9
- w_query: bfloat16 [2048, 1024], P(('sp', 'dp')), may hold values from -0.125 to 0.125
- w_key: bfloat16 [2048, 1024], P(('sp', 'dp')), may hold values from -0.125 to 0.125
- w_value: bfloat16 [2048, 2048], P(('sp', 'dp')), may hold values from -0.125 to 0.125
- w_out: bfloat16 [2048, 2048], P(('sp', 'dp')), may hold values from -0.125 to 0.125
- decay_rate: float32 [8, 8, 64], P('dp'), may hold values from 6.1035156e-06 to 0.08, as said below
Outputs:
- layer_out: bfloat16 [8, 8192, 2048], P('dp', 'sp')
The draws below stay inside these ranges and needn't reach their ends.
Inputs may be any that keep to these rules, and one draw needn't show every extreme that they name: `decay_rate`: one rate for each sequence, head and block of 128 positions.
All inputs are finite; a program needn't handle non-finite values.
Results may differ from the reference program's by a relative error of at most 0.02.
Values may be sent and summed in bfloat16 or wider, within the bound.
A program may use at most 128 MiB of HBM per device.

```python
import jax
import jax.numpy as jnp
from jax import lax

D = 2048
HEADS = 8
DK = 128
DV = 256
GROUP_W = 128
BLOCK = 128
SEQ = 8192
BATCH = 8


def draw_decay_rate(key, part):
    subkeys = jax.random.split(jax.random.fold_in(key, 17), 4)
    block_count = SEQ // BLOCK
    ranking = jax.vmap(lambda single: jax.random.permutation(single, HEADS))(jax.random.split(subkeys[0], BATCH))
    fast_count = HEADS // 2
    is_fast = ranking < fast_count
    slow_base = jnp.exp(jax.random.uniform(subkeys[1], (BATCH, HEADS), jnp.float32, jnp.log(0.1), jnp.log(0.5))) / SEQ
    fast_base = jnp.exp(jax.random.uniform(subkeys[2], (BATCH, HEADS), jnp.float32, jnp.log(0.02), jnp.log(0.04)))
    base_rate = jnp.where(is_fast, fast_base, slow_base)
    factor = jnp.exp(jax.random.uniform(subkeys[3], (BATCH, HEADS, block_count), jnp.float32, jnp.log(0.5), jnp.log(2.0)))
    return base_rate[:, :, None] * factor


def level_of(stream_key, dims, cuts, least, top_value):
    gain = 1.0
    for axis_at, blocks in cuts:
        heights = jax.random.uniform(jax.random.fold_in(jax.random.fold_in(stream_key, 6), axis_at), (blocks,), jnp.float32, least / len(cuts), top_value / len(cuts))
        gain = gain * jnp.repeat(jnp.exp(heights), dims[axis_at] // blocks).reshape((-1,) + (1,) * (len(dims) - 1 - axis_at))
    return gain


def gaussian(own_key, dims, scale, reach, cuts=(), kind=jnp.bfloat16):
    values = jax.random.normal(own_key, dims, jnp.float32) * scale
    if len(cuts) > 0:
        values = level_of(own_key, dims, cuts, -0.22, 0.18) * values
    return jnp.clip(values, min=-reach, max=reach).astype(kind)


def setup_inputs(seed: int = 0) -> dict:
    arg_keys = jax.random.split(jax.random.key(seed), 8)
    return {
        "tokens": gaussian(arg_keys[0], (BATCH, SEQ, D), 1.0, 6.0, ((0, 8), (1, 16))),
        "norm_gain": jnp.clip(1.0 + 0.18 * jax.random.normal(arg_keys[1], (D,), jnp.float32), 0.1, 1.9),
        "w_query": gaussian(arg_keys[2], (D, HEADS * DK), D ** -0.5, 0.125, ((0, 128),)),
        "w_key": gaussian(arg_keys[3], (D, HEADS * DK), D ** -0.5, 0.125, ((0, 128),)),
        "w_value": gaussian(arg_keys[4], (D, HEADS * DV), D ** -0.5, 0.125, ((0, 128),)),
        "w_out": gaussian(arg_keys[5], (HEADS * DV, D), (HEADS * DV) ** -0.5, 0.125, ((0, 128),)),
        "decay_rate": draw_decay_rate(jax.random.fold_in(arg_keys[7], 71), 0),
    }


EPS_RMS = 1e-06
EPS_GROUP = 0.01
ROPE_BASE = 10000.0

def rms_scaled(token_rows, norm_gain):
    widened = token_rows.astype(jnp.float32)
    inv_norm = lax.rsqrt(lax.optimization_barrier(jnp.mean(widened * widened, axis=-1, keepdims=True)) + EPS_RMS)
    return (widened * inv_norm * norm_gain).astype(jnp.bfloat16)

def rope_tables(length, head_depth):
    half_depth = head_depth // 2
    inverse = ROPE_BASE ** (-(jnp.arange(half_depth, dtype=jnp.float32) / (half_depth - 1)))
    angles = jnp.arange(length, dtype=jnp.float32)[:, None] * inverse[None, :]
    return (jnp.cos(angles), jnp.sin(angles))

def rotate(stacked, cosine_table, sine_table):
    paired = stacked.reshape(stacked.shape[0], stacked.shape[1], -1, 2)
    first_part = paired[..., 0]
    second_part = paired[..., 1]
    cos_rows = cosine_table[:, None, :]
    sin_rows = sine_table[:, None, :]
    turned = jnp.stack([first_part * cos_rows - second_part * sin_rows, second_part * cos_rows + first_part * sin_rows], axis=-1)
    return turned.reshape(stacked.shape)

def rounded_copy(widened):
    return lax.optimization_barrier(widened.astype(jnp.bfloat16)).astype(jnp.float32)

def retain(queries, keys_in, values_in, decay_rows):
    length, groups, head_depth = queries.shape
    channel_width = values_in.shape[-1]
    blocks = length // BLOCK

    def by_block(stacked):
        return stacked.astype(jnp.float32).reshape(blocks, BLOCK, groups, stacked.shape[-1]).transpose(2, 0, 1, 3)
    query_blocks = by_block(queries)
    key_blocks = by_block(keys_in)
    value_blocks = by_block(values_in)
    offsets = jnp.arange(BLOCK, dtype=jnp.float32)
    distance = offsets[:, None] - offsets[None, :]
    within = jnp.where(distance >= 0.0, jnp.exp(-decay_rows[:, :, None, None] * jnp.maximum(distance, 0.0)), 0.0)
    scores = jnp.einsum('gncd,gnmd->gncm', query_blocks, key_blocks)
    weighted = rounded_copy(scores * within)
    inner_sum = jnp.einsum('gncm,gnme->gnce', weighted, value_blocks)
    to_end = jnp.exp(-decay_rows[:, :, None] * (BLOCK - 1.0 - offsets))
    key_scaled = rounded_copy(key_blocks * to_end[..., None])
    local_state = jnp.einsum('gncd,gnce->gnde', key_scaled, value_blocks)
    carried = jnp.exp(-decay_rows * BLOCK)

    def advance(running, inputs):
        decay_now, added = inputs
        return (decay_now[:, None, None] * running + added, running)
    start_state = jnp.zeros((groups, head_depth, channel_width), jnp.float32)
    _, before = lax.scan(advance, start_state, (carried.T, local_state.transpose(1, 0, 2, 3)))
    from_start = jnp.exp(-decay_rows[:, :, None] * (offsets + 1.0))
    cross_term = jnp.einsum('gncd,ngde->gnce', query_blocks * from_start[..., None], before, precision=lax.Precision.HIGHEST)
    mixed = inner_sum + cross_term
    return mixed.transpose(1, 2, 0, 3).reshape(length, groups, channel_width)

def reference(tokens, norm_gain, w_query, w_key, w_value, w_out, decay_rate):

    def per_sequence(inputs):
        token_rows, decay_rows = inputs
        length = token_rows.shape[0]
        normed_in = rms_scaled(token_rows, norm_gain)
        query_proj = jnp.dot(normed_in, w_query, preferred_element_type=jnp.float32).astype(jnp.bfloat16)
        key_proj = jnp.dot(normed_in, w_key, preferred_element_type=jnp.float32).astype(jnp.bfloat16)
        value_proj = jnp.dot(normed_in, w_value, preferred_element_type=jnp.float32).astype(jnp.bfloat16)
        cosine_table, sine_table = rope_tables(length, DK)
        query_rot = rotate(query_proj.astype(jnp.float32).reshape(length, HEADS, DK), cosine_table, sine_table).astype(jnp.bfloat16)
        key_rot = (rotate(key_proj.astype(jnp.float32).reshape(length, HEADS, DK), cosine_table, sine_table) * DK ** (-0.5)).astype(jnp.bfloat16)
        mixed = retain(jnp.concatenate([query_rot, query_rot], axis=1), jnp.concatenate([key_rot, key_rot], axis=1), value_proj.reshape(length, 2 * HEADS, GROUP_W), jnp.concatenate([decay_rows, decay_rows], axis=0))
        halves = mixed.reshape(length, 2, HEADS, GROUP_W)
        mean_part = lax.optimization_barrier(jnp.sum(halves, axis=(1, 3), keepdims=True)) / DV
        square_part = lax.optimization_barrier(jnp.sum(halves * halves, axis=(1, 3), keepdims=True)) / DV
        retained = ((halves - mean_part) * lax.rsqrt(square_part - mean_part * mean_part + EPS_GROUP)).astype(jnp.bfloat16)
        return jnp.dot(retained.reshape(length, 2 * HEADS * GROUP_W), w_out, preferred_element_type=jnp.float32).astype(jnp.bfloat16)
    return lax.map(per_sequence, (tokens, decay_rate))
```

```python
import functools

import jax
import jax.numpy as jnp
import numpy as np
from jax import lax
from jax.experimental import pallas as pl
from jax.experimental.pallas import tpu as pltpu
from jax.sharding import Mesh
from jax.sharding import PartitionSpec as P

MESH = pl.DeviceIdType.MESH
F32 = jnp.float32
BF16 = jnp.bfloat16

HEADS = 8
DK = 128
DV = 256
BLOCK = 128
D = 2048
LEN = 512
SHARDS = 16
EPS_RMS = 1e-06
EPS_GROUP = 0.01
ROPE_BASE = 10000.0

K_PIECES = (0, 3)
V_PIECES = (1, 2, 4, 5)
Q_PIECES = (6, 7)
O_FIRST = 8
WAVES = 4
ORDERS = ((2, 1, 0), (1, 0, 2), (0, 2, 1))


def rope_constants():
    inverse = ROPE_BASE ** (-(np.arange(DK // 2, dtype=np.float64) / (DK // 2 - 1)))
    inverse = np.repeat(inverse, 2)
    high = np.arange(256, dtype=np.float64)[:, None] * 32 * inverse[None, :]
    low = np.arange(32, dtype=np.float64)[:, None] * inverse[None, :]
    high = np.stack([np.cos(high), np.sin(high)]).astype(np.float32)
    low = np.stack([np.cos(low), np.sin(low)]).astype(np.float32)
    return high, low


def kernel(
    tokens, gain, wq, wk, wv, wo, rates, high, low,
    out,
    w, x_raw, xn, rates2, cos_t, sin_t, rate_b, base_b, dec,
    keys, queries, values, s_send, s_recv, p_send, p_recv, ret, ret_send, out_v,
    tok_sem, own_sem, mate_s, mate_r, rate_s, rate_r, xn_s, xn_r,
    p1s, p1r, p2s, p2r, p2fs, p2fr, p3s, p3r, p3fs, p3fr,
    ss, sr, ps, pr, rs, rr, os, orr, out_sem,
):
    z, y, x, c = (lax.axis_index(a) for a in ("z", "y", "x", "c"))
    here = (z, y, x)
    shard = z * 4 + y
    mate = (z, y, x, 1 - c)

    def device(dim, step):
        at = list(here)
        at[dim] = lax.rem(at[dim] + step, 4)
        return (*at, c)

    def peer(step):
        to = lax.rem(shard + step, SHARDS)
        return to, (lax.div(to, 4), lax.rem(to, 4), x, c)

    tok_copies = []
    for i in range(4):
        rows = pl.ds(i * 128, 128)
        cp = pltpu.make_async_copy(tokens.at[0, rows], x_raw.at[rows], tok_sem.at[i])
        tok_copies.append(cp)

    def pieces_of(wave, core):
        todo = []
        for piece in range(3 * wave, 3 * wave + 3):
            if piece in K_PIECES or piece in Q_PIECES:
                ref = wk if piece in K_PIECES else wq
                j = K_PIECES.index(piece) if piece in K_PIECES else Q_PIECES.index(piece)
                at = pl.multiple_of(core * 512 + j * 256, 256)
                todo.append((ref.at[:, pl.ds(at, 256)], piece, pl.ds(0, 256)))
            elif piece in V_PIECES:
                h = V_PIECES.index(piece)
                for s in range(2):
                    at = pl.multiple_of(core * 512 + (s * 1024 + h * 128), 128)
                    todo.append((wv.at[:, pl.ds(at, 128)], piece, pl.ds(s * 128, 128)))
            else:
                at = pl.multiple_of(core * 1024 + (piece - O_FIRST) * 256, 256)
                todo.append((wo.at[:, pl.ds(at, 256)], piece, pl.ds(0, 256)))
        return todo

    own_rows = pl.ds(pl.multiple_of(c * 16, 16), 16)
    for wave in range(WAVES):
        for src, piece, cols in pieces_of(wave, c):
            pltpu.make_async_copy(src, w.at[piece, z, y, x, own_rows, cols], own_sem.at[wave]).start()
        if wave == 0:
            for cp in tok_copies:
                cp.start()

    barrier = pltpu.get_barrier_semaphore()

    def greet(step, carry):
        _, dev = peer(step)
        pl.semaphore_signal(barrier, inc=1, device_id=dev, device_id_type=MESH)
        return carry

    lax.fori_loop(1, SHARDS, greet, 0)
    for step in range(1, 4):
        pl.semaphore_signal(barrier, inc=1, device_id=device(2, step), device_id_type=MESH)
    pl.semaphore_signal(barrier, inc=1, device_id=mate, device_id_type=MESH)
    pl.semaphore_wait(barrier, 19)

    for wave in range(WAVES):
        for src, piece, cols in pieces_of(wave, 1 - c):
            pltpu.make_async_remote_copy(
                src, w.at[piece, z, y, x, own_rows, cols],
                mate_s.at[wave], mate_r.at[wave], device_id=mate, device_id_type=MESH,
            ).start()
        if wave == 0:
            rate_copy = pltpu.make_async_remote_copy(
                rates, rates2, rate_s, rate_r, device_id=mate, device_id_type=MESH
            )
            rate_copy.start()

    def part_slice(piece, where):
        idx = tuple(where.get(d, pl.ds(0, 4)) for d in range(3))
        return w.at[(piece, *idx)]

    def send(src, ssem, rsem, dev):
        pltpu.make_async_remote_copy(src, src, ssem, rsem, device_id=dev, device_id_type=MESH).start()

    def drain(ref, sem):
        pltpu.make_async_copy(ref, ref, sem).wait()

    def three(wave):
        return pl.ds(3 * wave, 3)

    def p1_wait_ref(wave):
        return w.at[three(wave), 0, 0, pl.ds(0, 3)]

    def p2_wait_ref(wave):
        return w.at[three(wave), pl.ds(0, 2), 0]

    def p2f_wait_ref(wave):
        return w.at[three(wave), 0, 0]

    def half_wait_ref(wave):
        return w.at[3 * wave, pl.ds(0, 2), 0]

    HALF = (pl.ds(0, 2), pl.ds(2, 2))

    def stage_p0(wave):
        ref = w.at[three(wave), 0, 0, 0, pl.ds(0, 16)]
        drain(ref, own_sem.at[wave])
        drain(ref, mate_r.at[wave])
        for part, (d1, d2, d3) in enumerate(ORDERS):
            piece = 3 * wave + part
            own = part_slice(piece, {0: z, 1: y, 2: x})
            for step in (1, 3, 2):
                send(own, p1s.at[wave], p1r.at[wave], device(d1, step))

    def stage_a(wave):
        drain(p1_wait_ref(wave), p1r.at[wave])
        for part, (d1, d2, d3) in enumerate(ORDERS):
            own = part_slice(3 * wave + part, {d2: here[d2], d3: here[d3]})
            for step in (1, 3):
                send(own, p2s.at[wave], p2r.at[wave], device(d2, step))

    def stage_b(wave):
        drain(p2_wait_ref(wave), p2r.at[wave])
        for part, (d1, d2, d3) in enumerate(ORDERS):
            for i, step in enumerate((1, 3)):
                origin = lax.rem(here[d2] + 4 - step, 4)
                src = part_slice(3 * wave + part, {d1: HALF[i], d2: origin, d3: here[d3]})
                send(src, p2fs.at[wave], p2fr.at[wave], device(d2, step))

    def stage_c(wave):
        drain(p2f_wait_ref(wave), p2fr.at[wave])
        for sub in range(2):
            for part, (d1, d2, d3) in enumerate(ORDERS):
                for i, step in enumerate((1, 3)):
                    half = sub if i == 0 else 1 - sub
                    src = part_slice(3 * wave + part, {d2: HALF[half], d3: here[d3]})
                    send(src, p3s.at[wave], p3r.at[wave, part, i, sub], device(d3, step))

    def stage_d(wave):
        for part, (d1, d2, d3) in enumerate(ORDERS):
            for i, step in enumerate((1, 3)):
                drain(half_wait_ref(wave), p3r.at[wave, part, i, 0])
                origin = lax.rem(here[d3] + 4 - step, 4)
                src = part_slice(3 * wave + part, {d2: HALF[i], d3: origin})
                send(src, p3fs.at[wave], p3fr.at[wave, part, i], device(d3, step))

    def stage_e(wave):
        for part in range(3):
            for i in range(2):
                drain(half_wait_ref(wave), p3r.at[wave, part, i, 1])
                drain(half_wait_ref(wave), p3fr.at[wave, part, i])

    def finish_sends(wave):
        drain(w.at[three(wave), 0, 0, 0, pl.ds(0, 16)], mate_s.at[wave])
        drain(p1_wait_ref(wave), p1s.at[wave])
        drain(p2_wait_ref(wave), p2s.at[wave])
        drain(p2f_wait_ref(wave), p2fs.at[wave])
        drain(w.at[three(wave), pl.ds(0, 2)], p3s.at[wave])
        drain(w.at[three(wave), 0], p3fs.at[wave])

    def norm(i):
        rows = pl.ds(i * 128, 128)
        tok_copies[i].wait()
        wide = x_raw[rows].astype(F32)
        inv = lax.rsqrt(jnp.sum(wide * wide, axis=-1, keepdims=True) * (1.0 / D) + EPS_RMS)
        xn[0, rows] = (wide * inv * gain[...]).astype(BF16)

    def norm_copy(i):
        rows = pl.ds(i * 128, 128)
        return pltpu.make_async_remote_copy(
            xn.at[0, rows], xn.at[1, rows], xn_s.at[i], xn_r.at[i], device_id=mate, device_id_type=MESH
        )

    def tables():
        lane = lax.broadcasted_iota(jnp.int32, (32, DK), 1)
        sign = jnp.where(lax.rem(lane, 2) == 0, -1.0, 1.0).astype(F32)
        cl, sl = low[0], low[1]
        for i in range(16):
            at = shard * 16 + i
            ch, sh = high[0, pl.ds(at, 1)], high[1, pl.ds(at, 1)]
            cos_t[pl.ds(i * 32, 32)] = ch * cl - sh * sl
            sin_t[pl.ds(i * 32, 32)] = (sh * cl + ch * sl) * sign

    def decays():
        lane = lax.broadcasted_iota(jnp.int32, (4, 64), 1)
        for s in range(2):
            full = rates[...] if s == 0 else rates2[...]
            mine = jnp.where(c == 0, full[0:4], full[4:8])
            base = jnp.zeros((4, 1), F32)
            for n in range(4):
                r = jnp.sum(jnp.where(lane == shard * 4 + n, mine, 0.0), axis=1, keepdims=True)
                rate_b[s, n] = jnp.broadcast_to(r, (4, 128))
                base_b[s, n] = jnp.broadcast_to(base, (4, 128))
                base = base + r * float(BLOCK)
            base_b[s, 4] = jnp.broadcast_to(base, (4, 128))
            for t in range(SHARDS - 1):
                tot = jnp.sum(jnp.where(lax.div(lane, 4) == t, mine, 0.0), axis=1, keepdims=True)
                e = jnp.broadcast_to(jnp.exp(tot * (-float(BLOCK))), (4, 128))
                for h in range(4):
                    dec[h // 2, s * 2 + h % 2, pl.ds(t, 1)] = e[h : h + 1]

    def turned(prod, s, h, sign, scale):
        v = prod.astype(BF16).astype(F32)
        even = lax.rem(lax.broadcasted_iota(jnp.int32, v.shape, 1), 2) == 0
        swap = jnp.where(even, pltpu.roll(v, DK - 1, 1), pltpu.roll(v, 1, 1))
        rot = v * cos_t[...] + swap * sin_t[...]
        offset = (lax.broadcasted_iota(jnp.int32, (BLOCK, DK), 0) + 1).astype(F32)
        parts = []
        for n in range(4):
            e = base_b[s, n, pl.ds(h, 1)] + rate_b[s, n, pl.ds(h, 1)] * offset
            parts.append(rot[n * BLOCK : (n + 1) * BLOCK] * (jnp.exp(e * sign) * scale))
        return jnp.concatenate(parts, axis=0).astype(BF16)

    def project(s, piece):
        return jnp.dot(xn[s], w[piece].reshape(D, 256), preferred_element_type=F32)

    def key_piece(j):
        def body(s, carry):
            prod = project(s, K_PIECES[j])
            for hh in range(2):
                h = 2 * j + hh
                keys[s, h] = turned(prod[:, hh * 128 : (hh + 1) * 128], s, h, 1.0, DK ** (-0.5))
            return carry
        lax.fori_loop(0, 2, body, 0)

    def query_piece(j):
        def body(s, carry):
            prod = project(s, Q_PIECES[j])
            for hh in range(2):
                h = 2 * j + hh
                queries[s, h] = turned(prod[:, hh * 128 : (hh + 1) * 128], s, h, -1.0, 1.0)
            return carry
        lax.fori_loop(0, 2, body, 0)

    def value_piece(h):
        def body(s, carry):
            values[s, h] = project(s, V_PIECES[h]).astype(BF16)
            return carry
        lax.fori_loop(0, 2, body, 0)

    def local_states(half):
        def body(p, carry):
            s, h = lax.div(p, 2), half * 2 + lax.rem(p, 2)
            st = lax.dot_general(
                keys[s, h], values[s, h], (((0,), (0,)), ((), ())), preferred_element_type=F32
            )
            e = jnp.exp(-base_b[s, 4, pl.ds(h, 1)])
            e = jnp.concatenate([e, e], axis=1)
            s_send[half, pl.ds(p * 4, 4)] = (st * e).astype(BF16).reshape(4, 32, DV)
            return carry
        lax.fori_loop(0, 4, body, 0)
        s_recv[half, shard] = s_send[half, shard]

    def send_states(half):
        def body(step, carry):
            to, dev = peer(step)
            pltpu.make_async_remote_copy(
                s_send.at[half, to], s_recv.at[half, shard], ss.at[half], sr.at[half],
                device_id=dev, device_id_type=MESH,
            ).start()
            return carry
        lax.fori_loop(1, SHARDS, body, 0)

    def scan_states(half):
        drain(s_recv.at[half, pl.ds(0, SHARDS - 1)], sr.at[half])
        run = jnp.zeros((32, DV), F32)
        rows = dec[half, z]
        for t in range(SHARDS):
            p_send[half, t] = run.astype(BF16)
            if t < SHARDS - 1:
                e = rows[t : t + 1]
                run = run * jnp.concatenate([e, e], axis=1) + s_recv[half, t].astype(F32)
        p_recv[half, shard] = p_send[half, shard]

    def send_prefixes(half):
        def body(step, carry):
            to, dev = peer(step)
            pltpu.make_async_remote_copy(
                p_send.at[half, to], p_recv.at[half, shard], ps.at[half], pr.at[half],
                device_id=dev, device_id_type=MESH,
            ).start()
            return carry
        lax.fori_loop(1, SHARDS, body, 0)

    def retention(s, half):
        row = lax.broadcasted_iota(jnp.int32, (256, 256), 0)
        col = lax.broadcasted_iota(jnp.int32, (256, 256), 1)
        def body(hh, carry):
            h = half * 2 + hh
            p = s * 2 + hh
            before = p_recv[half, pl.ds(p * 4, 4)].reshape(DK, DV)
            for i in range(2):
                q = queries[s, h, pl.ds(i * 256, 256)]
                mixed = jnp.dot(q, before, preferred_element_type=F32)
                for j in range(i + 1):
                    k = keys[s, h, pl.ds(j * 256, 256)]
                    sc = lax.dot_general(q, k, (((1,), (1,)), ((), ())), preferred_element_type=F32)
                    if i == j:
                        sc = jnp.where(row >= col, sc, 0.0)
                    mixed = mixed + jnp.dot(
                        sc.astype(BF16), values[s, h, pl.ds(j * 256, 256)], preferred_element_type=F32
                    )
                mu = jnp.sum(mixed, axis=1, keepdims=True) * (1.0 / DV)
                sq = jnp.sum(mixed * mixed, axis=1, keepdims=True) * (1.0 / DV)
                done = ((mixed - mu) * lax.rsqrt(sq - mu * mu + EPS_GROUP)).astype(BF16)
                rows = pl.ds(i * 256, 256)
                if s == 0:
                    for g in range(2):
                        at = pl.multiple_of((g * HEADS + c * 4 + h) * 128, 128)
                        ret[rows, pl.ds(at, 128)] = done[:, g * 128 : (g + 1) * 128]
                else:
                    ret_send[h, rows] = done
            if s == 1:
                for g in range(2):
                    at = pl.multiple_of((g * HEADS + c * 4 + h) * 128, 128)
                    pltpu.make_async_remote_copy(
                        ret_send.at[h, :, pl.ds(g * 128, 128)], ret.at[:, pl.ds(at, 128)],
                        rs.at[h], rr.at[h], device_id=mate, device_id_type=MESH,
                    ).start()
            return carry
        lax.fori_loop(0, 2, body, 0)

    def pass_out(piece):
        j = piece - O_FIRST
        pltpu.make_async_remote_copy(
            w.at[piece], w.at[piece + 4], os.at[j], orr.at[j], device_id=mate, device_id_type=MESH
        ).start()

    def out_copy(j, core):
        at = pl.multiple_of(core * 1024 + j * 256, 256)
        slot = j if core is c else j + 4
        return pltpu.make_async_copy(out_v.at[slot], out.at[0, :, pl.ds(at, 256)], out_sem.at[slot])

    def out_pieces(core):
        first = O_FIRST if core is c else O_FIRST + 4
        def body(j, carry):
            if core is not c:
                drain(w.at[0], orr.at[j])
            prod = jnp.dot(ret[...], w[first + j].reshape(D, 256), preferred_element_type=F32)
            out_v[first - O_FIRST + j] = prod.astype(BF16)
            out_copy(j, core).start()
            return carry
        lax.fori_loop(0, 4, body, 0)

    other = 1 - c

    tables()
    stage_p0(0)
    stage_p0(1)
    norm(0)
    stage_a(0)
    norm(1)
    norm_copy(0).start()
    stage_a(1)
    norm(2)
    norm_copy(1).start()
    stage_b(0)
    norm(3)
    norm_copy(2).start()
    stage_b(1)
    stage_p0(2)
    stage_p0(3)
    norm_copy(3).start()
    stage_c(0)
    rate_copy.wait()
    decays()
    stage_a(2)
    stage_a(3)
    stage_d(0)
    stage_c(1)
    stage_b(2)
    stage_b(3)
    for i in range(4):
        norm_copy(i).wait()
    stage_e(0)
    key_piece(0)
    value_piece(0)
    value_piece(1)
    local_states(0)
    stage_d(1)
    send_states(0)
    stage_c(2)
    stage_e(1)
    key_piece(1)
    value_piece(2)
    value_piece(3)
    local_states(1)
    scan_states(0)
    send_states(1)
    stage_d(2)
    send_prefixes(0)
    stage_c(3)
    stage_e(2)
    pass_out(O_FIRST)
    query_piece(0)
    scan_states(1)
    query_piece(1)
    send_prefixes(1)
    drain(p_recv.at[0, pl.ds(0, SHARDS - 1)], pr.at[0])
    retention(1, 0)
    stage_d(3)
    retention(0, 0)
    drain(p_recv.at[1, pl.ds(0, SHARDS - 1)], pr.at[1])
    retention(1, 1)
    retention(0, 1)
    stage_e(3)
    for piece in range(O_FIRST + 1, O_FIRST + 4):
        pass_out(piece)
    for h in range(4):
        drain(ret_send.at[0], rr.at[h])
    out_pieces(c)
    out_pieces(other)

    for wave in range(WAVES):
        finish_sends(wave)
    for half in range(2):
        drain(s_recv.at[half, pl.ds(0, SHARDS - 1)], ss.at[half])
        drain(p_recv.at[half, pl.ds(0, SHARDS - 1)], ps.at[half])
    for h in range(4):
        drain(ret_send.at[0], rs.at[h])
        drain(w.at[0], os.at[h])
    for j in range(4):
        out_copy(j, c).wait()
        out_copy(j, other).wait()


def body(tokens, norm_gain, w_query, w_key, w_value, w_out, decay_rate):
    high, low = rope_constants()
    any_spec = pl.BlockSpec(memory_space=pl.ANY)
    vmem = pl.BlockSpec(memory_space=pltpu.VMEM)
    dma = pltpu.SemaphoreType.DMA
    scratch = [
        pltpu.VMEM((16, 4, 4, 4, 32, 256), BF16),
        pltpu.VMEM((LEN, D), BF16),
        pltpu.VMEM((2, LEN, D), BF16),
        pltpu.VMEM((HEADS, 64), F32),
        pltpu.VMEM((LEN, DK), F32),
        pltpu.VMEM((LEN, DK), F32),
        pltpu.VMEM((2, 4, 4, 128), F32),
        pltpu.VMEM((2, 5, 4, 128), F32),
        pltpu.VMEM((2, 4, SHARDS, 128), F32),
        pltpu.VMEM((2, 4, LEN, DK), BF16),
        pltpu.VMEM((2, 4, LEN, DK), BF16),
        pltpu.VMEM((2, 4, LEN, DV), BF16),
        pltpu.VMEM((2, SHARDS, 32, DV), BF16),
        pltpu.VMEM((2, SHARDS, 32, DV), BF16),
        pltpu.VMEM((2, SHARDS, 32, DV), BF16),
        pltpu.VMEM((2, SHARDS, 32, DV), BF16),
        pltpu.VMEM((LEN, D), BF16),
        pltpu.VMEM((4, LEN, DV), BF16),
        pltpu.VMEM((8, LEN, 256), BF16),
        dma((4,)), dma((WAVES,)), dma((WAVES,)), dma((WAVES,)), dma, dma, dma((4,)), dma((4,)),
        dma((WAVES,)), dma((WAVES,)), dma((WAVES,)), dma((WAVES,)), dma((WAVES,)), dma((WAVES,)),
        dma((WAVES,)), dma((WAVES, 3, 2, 2)), dma((WAVES,)), dma((WAVES, 3, 2)),
        dma((2,)), dma((2,)), dma((2,)), dma((2,)), dma((4,)), dma((4,)), dma((4,)), dma((4,)), dma((8,)),
    ]
    return pl.pallas_call(
        kernel,
        out_shape=jax.ShapeDtypeStruct((1, LEN, D), BF16),
        in_specs=[any_spec, vmem, any_spec, any_spec, any_spec, any_spec, vmem, vmem, vmem],
        out_specs=any_spec,
        scratch_shapes=scratch,
        compiler_params=pltpu.CompilerParams(
            collective_id=0, has_side_effects=True, vmem_limit_bytes=60 * 1024 * 1024
        ),
    )(tokens, norm_gain[None], w_query, w_key, w_value, w_out, decay_rate[0], jnp.asarray(high), jnp.asarray(low))


def solution(mesh):
    split = Mesh(mesh.devices.reshape(4, 4, 4, 2), ("z", "y", "x", "c"))
    in_specs = (
        P(("x", "c"), ("z", "y"), None),
        P(),
        P(("z", "y", "x", "c"), None),
        P(("z", "y", "x", "c"), None),
        P(("z", "y", "x", "c"), None),
        P(("z", "y", "x", "c"), None),
        P(("x", "c"), None, None),
    )
    return jax.shard_map(
        body, mesh=split, in_specs=in_specs, out_specs=P(("x", "c"), ("z", "y"), None), check_vma=False
    )
```

```python
import functools

import jax
import jax.numpy as jnp
import numpy as np
from jax import lax
from jax.experimental import pallas as pl
from jax.experimental.pallas import tpu as pltpu
from jax.sharding import Mesh
from jax.sharding import PartitionSpec as P

MESH = pl.DeviceIdType.MESH
F32 = jnp.float32
BF16 = jnp.bfloat16

HEADS = 8
DK = 128
DV = 256
BLOCK = 128
D = 2048
LEN = 512
SHARDS = 16
EPS_RMS = 1e-06
EPS_GROUP = 0.01
ROPE_BASE = 10000.0

K_PIECES = (0, 3)
V_PIECES = (1, 2, 4, 5)
Q_PIECES = (6, 7)
O_FIRST = 8
WAVES = 4
ORDERS = (
    ((2, 1, 0), (1, 0, 2), (0, 2, 1)),
    ((2, 1, 0), (1, 0, 2), (0, 2, 1)),
    ((1, 2, 0), (0, 1, 2), (2, 0, 1)),
    ((0, 2, 1), (1, 2, 0), (0, 1, 2)),
)


def rope_constants():
    inverse = ROPE_BASE ** (-(np.arange(DK // 2, dtype=np.float64) / (DK // 2 - 1)))
    inverse = np.repeat(inverse, 2)
    high = np.arange(256, dtype=np.float64)[:, None] * 32 * inverse[None, :]
    low = np.arange(32, dtype=np.float64)[:, None] * inverse[None, :]
    high = np.stack([np.cos(high), np.sin(high)]).astype(np.float32)
    low = np.stack([np.cos(low), np.sin(low)]).astype(np.float32)
    return high, low


def kernel(
    tokens, gain_in, wq, wk, wv, wo, rates_in, high_in, low_in,
    out,
    w, for_mate, x_raw, xn, gain, high, low, rates, rates2, cos_t, sin_t, rate_b, base_b, dec,
    keys, queries, values, s_send, s_recv, p_send, p_recv, ret, ret_send, out_v,
    in_sem, tok_sem, own_sem, mate_s, mate_r, rate_s, rate_r, xn_s, xn_r,
    p1s, p1r, p2s, p2r, p2fs, p2fr, p3s, p3r, p3fs, p3fr,
    ss, sr, ps, pr, rs, rr, os, orr, out_sem,
):
    z, y, x, c = (lax.axis_index(a) for a in ("z", "y", "x", "c"))
    here = (z, y, x)
    shard = z * 4 + y
    mate = (z, y, x, 1 - c)

    def device(dim, step, core=None):
        at = list(here)
        at[dim] = lax.rem(at[dim] + step, 4)
        return (*at, c if core is None else core)

    def peer(step):
        to = lax.rem(shard + step, SHARDS)
        return to, (lax.div(to, 4), lax.rem(to, 4), x, c)

    tok_copies = []
    for i in range(4):
        rows = pl.ds(i * 128, 128)
        cp = pltpu.make_async_copy(tokens.at[0, rows], x_raw.at[rows], tok_sem.at[i])
        tok_copies.append(cp)

    def pieces_of(wave, core):
        todo = []
        for piece in range(3 * wave, 3 * wave + 3):
            if piece in K_PIECES or piece in Q_PIECES:
                ref = wk if piece in K_PIECES else wq
                j = K_PIECES.index(piece) if piece in K_PIECES else Q_PIECES.index(piece)
                at = pl.multiple_of(core * 512 + j * 256, 256)
                todo.append((ref.at[:, pl.ds(at, 256)], piece, pl.ds(0, 256)))
            elif piece in V_PIECES:
                h = V_PIECES.index(piece)
                for s in range(2):
                    at = pl.multiple_of(core * 512 + (s * 1024 + h * 128), 128)
                    todo.append((wv.at[:, pl.ds(at, 128)], piece, pl.ds(s * 128, 128)))
            else:
                at = pl.multiple_of(core * 1024 + (piece - O_FIRST) * 256, 256)
                todo.append((wo.at[:, pl.ds(at, 256)], piece, pl.ds(0, 256)))
        return todo

    own_rows = pl.ds(pl.multiple_of(c * 16, 16), 16)
    other = 1 - c

    barrier = pltpu.get_barrier_semaphore()
    first_peers = [mate]
    for dim in range(3):
        for step in (1, 3, 2):
            first_peers += [device(dim, step), device(dim, step, other)]
    for dev in first_peers:
        pl.semaphore_signal(barrier, inc=1, device_id=dev, device_id_type=MESH)

    in_copies = [
        pltpu.make_async_copy(gain_in, gain, in_sem.at[0]),
        pltpu.make_async_copy(rates_in, rates, in_sem.at[1]),
        pltpu.make_async_copy(high_in.at[:, pl.ds(pl.multiple_of(shard * 16, 16), 16)], high, in_sem.at[2]),
        pltpu.make_async_copy(low_in, low, in_sem.at[3]),
    ]
    for cp in in_copies + tok_copies:
        cp.start()
    for wave in range(WAVES):
        for src, piece, cols in pieces_of(wave, c):
            pltpu.make_async_copy(src, w.at[piece, z, y, x, own_rows, cols], own_sem.at[wave]).start()
        for src, piece, cols in pieces_of(wave, other):
            pltpu.make_async_copy(src, for_mate.at[piece, :, cols], own_sem.at[wave]).start()
    pl.semaphore_wait(barrier, len(first_peers))
    rate_copy = pltpu.make_async_remote_copy(
        rates_in, rates2, rate_s, rate_r, device_id=mate, device_id_type=MESH
    )

    def part_slice(piece, where):
        idx = tuple(where.get(d, pl.ds(0, 4)) for d in range(3))
        return w.at[(piece, *idx)]

    def send(src, ssem, rsem, dev):
        pltpu.make_async_remote_copy(src, src, ssem, rsem, device_id=dev, device_id_type=MESH).start()

    def drain(ref, sem):
        pltpu.make_async_copy(ref, ref, sem).wait()

    def three(wave):
        return pl.ds(3 * wave, 3)

    def p1_wait_ref(wave):
        return w.at[three(wave), 0, 0, pl.ds(0, 3)]

    def p2_wait_ref(wave):
        return w.at[three(wave), pl.ds(0, 2), 0]

    def p2f_wait_ref(wave):
        return w.at[three(wave), 0, 0]

    def half_wait_ref(wave):
        return w.at[3 * wave, pl.ds(0, 2), 0]

    HALF = (pl.ds(0, 2), pl.ds(2, 2))

    def stage_p(wave):
        drain(w.at[three(wave), 0, 0, 0], own_sem.at[wave])
        for part, (d1, d2, d3) in enumerate(ORDERS[wave]):
            piece = 3 * wave + part
            own = w.at[piece, z, y, x, own_rows]
            pltpu.make_async_remote_copy(
                for_mate.at[piece], own, mate_s.at[wave], mate_r.at[wave], device_id=mate, device_id_type=MESH
            ).start()
            for step in (1, 3, 2):
                for src, core in ((own, c), (for_mate.at[piece], other)):
                    pltpu.make_async_remote_copy(
                        src, own, p1s.at[wave], p1r.at[wave],
                        device_id=device(d1, step, core), device_id_type=MESH,
                    ).start()

    def stage_a(wave):
        drain(w.at[three(wave), 0, 0, 0, pl.ds(0, 16)], mate_r.at[wave])
        drain(p1_wait_ref(wave), p1r.at[wave])
        for part, (d1, d2, d3) in enumerate(ORDERS[wave]):
            own = part_slice(3 * wave + part, {d2: here[d2], d3: here[d3]})
            for step in (1, 3):
                send(own, p2s.at[wave], p2r.at[wave], device(d2, step))

    def stage_b(wave):
        drain(p2_wait_ref(wave), p2r.at[wave])
        for part, (d1, d2, d3) in enumerate(ORDERS[wave]):
            for i, step in enumerate((1, 3)):
                origin = lax.rem(here[d2] + 4 - step, 4)
                src = part_slice(3 * wave + part, {d1: HALF[i], d2: origin, d3: here[d3]})
                send(src, p2fs.at[wave], p2fr.at[wave], device(d2, step))

    def stage_c(wave):
        drain(p2f_wait_ref(wave), p2fr.at[wave])
        for sub in range(2):
            for part, (d1, d2, d3) in enumerate(ORDERS[wave]):
                for i, step in enumerate((1, 3)):
                    half = sub if i == 0 else 1 - sub
                    src = part_slice(3 * wave + part, {d2: HALF[half], d3: here[d3]})
                    send(src, p3s.at[wave], p3r.at[wave, part, i, sub], device(d3, step))
        for part in range(3):
            if 3 * wave + part >= O_FIRST:
                d3 = ORDERS[wave][part][2]
                pass_on(3 * wave + part, d3, here[d3])

    def stage_d(wave, part):
        d1, d2, d3 = ORDERS[wave][part]
        for i, step in enumerate((1, 3)):
            drain(half_wait_ref(wave), p3r.at[wave, part, i, 0])
            origin = lax.rem(here[d3] + 4 - step, 4)
            src = part_slice(3 * wave + part, {d2: HALF[i], d3: origin})
            send(src, p3fs.at[wave, part], p3fr.at[wave, part, i], device(d3, step))

    def pass_on(piece, d3, at):
        j = piece - O_FIRST
        pltpu.make_async_remote_copy(
            part_slice(piece, {d3: at}), part_slice(piece + 4, {d3: at}),
            os.at[j], orr.at[j], device_id=mate, device_id_type=MESH,
        ).start()

    def stage_e(wave, part):
        piece = 3 * wave + part
        d3 = ORDERS[wave][part][2]
        for i, step in enumerate((1, 3)):
            drain(half_wait_ref(wave), p3r.at[wave, part, i, 1])
            if piece >= O_FIRST:
                pass_on(piece, d3, lax.rem(here[d3] + 4 - step, 4))

    def stage_f(wave, part):
        piece = 3 * wave + part
        d3 = ORDERS[wave][part][2]
        for i in range(2):
            drain(half_wait_ref(wave), p3fr.at[wave, part, i])
        if piece >= O_FIRST:
            pass_on(piece, d3, lax.rem(here[d3] + 2, 4))

    def finish_sends(wave):
        drain(w.at[three(wave), 0, 0, 0, pl.ds(0, 16)], mate_s.at[wave])
        drain(p1_wait_ref(wave), p1s.at[wave])
        drain(p2_wait_ref(wave), p2s.at[wave])
        drain(p2f_wait_ref(wave), p2fs.at[wave])
        drain(w.at[three(wave), pl.ds(0, 2)], p3s.at[wave])
        for part in range(3):
            drain(w.at[3 * wave, 0], p3fs.at[wave, part])

    def norm(i):
        rows = pl.ds(i * 128, 128)
        tok_copies[i].wait()
        wide = x_raw[rows].astype(F32)
        inv = lax.rsqrt(jnp.sum(wide * wide, axis=-1, keepdims=True) * (1.0 / D) + EPS_RMS)
        xn[0, rows] = (wide * inv * gain[...]).astype(BF16)

    def norm_copy(i):
        rows = pl.ds(i * 128, 128)
        return pltpu.make_async_remote_copy(
            xn.at[0, rows], xn.at[1, rows], xn_s.at[i], xn_r.at[i], device_id=mate, device_id_type=MESH
        )

    def tables():
        lane = lax.broadcasted_iota(jnp.int32, (32, DK), 1)
        sign = jnp.where(lax.rem(lane, 2) == 0, -1.0, 1.0).astype(F32)
        cl, sl = low[0], low[1]
        for i in range(16):
            ch, sh = high[0, pl.ds(i, 1)], high[1, pl.ds(i, 1)]
            cos_t[pl.ds(i * 32, 32)] = ch * cl - sh * sl
            sin_t[pl.ds(i * 32, 32)] = (sh * cl + ch * sl) * sign

    def decays():
        lane = lax.broadcasted_iota(jnp.int32, (4, 64), 1)
        for s in range(2):
            full = rates[...] if s == 0 else rates2[...]
            mine = jnp.where(c == 0, full[0:4], full[4:8])
            base = jnp.zeros((4, 1), F32)
            for n in range(4):
                r = jnp.sum(jnp.where(lane == shard * 4 + n, mine, 0.0), axis=1, keepdims=True)
                rate_b[s, n] = jnp.broadcast_to(r, (4, 128))
                base_b[s, n] = jnp.broadcast_to(base, (4, 128))
                base = base + r * float(BLOCK)
            base_b[s, 4] = jnp.broadcast_to(base, (4, 128))
            for t in range(SHARDS - 1):
                tot = jnp.sum(jnp.where(lax.div(lane, 4) == t, mine, 0.0), axis=1, keepdims=True)
                e = jnp.broadcast_to(jnp.exp(tot * (-float(BLOCK))), (4, 128))
                for h in range(4):
                    dec[h // 2, s * 2 + h % 2, pl.ds(t, 1)] = e[h : h + 1]

    def turned(prod, s, h, sign, scale):
        v = prod.astype(BF16).astype(F32)
        even = lax.rem(lax.broadcasted_iota(jnp.int32, v.shape, 1), 2) == 0
        swap = jnp.where(even, pltpu.roll(v, DK - 1, 1), pltpu.roll(v, 1, 1))
        rot = v * cos_t[...] + swap * sin_t[...]
        offset = (lax.broadcasted_iota(jnp.int32, (BLOCK, DK), 0) + 1).astype(F32)
        parts = []
        for n in range(4):
            e = base_b[s, n, pl.ds(h, 1)] + rate_b[s, n, pl.ds(h, 1)] * offset
            parts.append(rot[n * BLOCK : (n + 1) * BLOCK] * (jnp.exp(e * sign) * scale))
        return jnp.concatenate(parts, axis=0).astype(BF16)

    def project(s, piece):
        return jnp.dot(xn[s], w[piece].reshape(D, 256), preferred_element_type=F32)

    def key_piece(j):
        def body(s, carry):
            prod = project(s, K_PIECES[j])
            for hh in range(2):
                h = 2 * j + hh
                keys[s, h] = turned(prod[:, hh * 128 : (hh + 1) * 128], s, h, 1.0, DK ** (-0.5))
            return carry
        lax.fori_loop(0, 2, body, 0)

    def query_piece(j):
        def body(s, carry):
            prod = project(s, Q_PIECES[j])
            for hh in range(2):
                h = 2 * j + hh
                queries[s, h] = turned(prod[:, hh * 128 : (hh + 1) * 128], s, h, -1.0, 1.0)
            return carry
        lax.fori_loop(0, 2, body, 0)

    def value_piece(h):
        def body(s, carry):
            values[s, h] = project(s, V_PIECES[h]).astype(BF16)
            return carry
        lax.fori_loop(0, 2, body, 0)

    def local_states(half):
        def body(p, carry):
            s, h = lax.div(p, 2), half * 2 + lax.rem(p, 2)
            st = lax.dot_general(
                keys[s, h], values[s, h], (((0,), (0,)), ((), ())), preferred_element_type=F32
            )
            e = jnp.exp(-base_b[s, 4, pl.ds(h, 1)])
            e = jnp.concatenate([e, e], axis=1)
            s_send[half, pl.ds(p * 4, 4)] = (st * e).astype(BF16).reshape(4, 32, DV)
            return carry
        lax.fori_loop(0, 4, body, 0)
        s_recv[half, shard] = s_send[half, shard]

    def send_states(half):
        def body(step, carry):
            to, dev = peer(step)
            pltpu.make_async_remote_copy(
                s_send.at[half, to], s_recv.at[half, shard], ss.at[half], sr.at[half],
                device_id=dev, device_id_type=MESH,
            ).start()
            return carry
        lax.fori_loop(1, SHARDS, body, 0)

    def scan_states(half):
        drain(s_recv.at[half, pl.ds(0, SHARDS - 1)], sr.at[half])
        run = jnp.zeros((32, DV), F32)
        rows = dec[half, z]
        for t in range(SHARDS):
            p_send[half, t] = run.astype(BF16)
            if t < SHARDS - 1:
                e = rows[t : t + 1]
                run = run * jnp.concatenate([e, e], axis=1) + s_recv[half, t].astype(F32)
        p_recv[half, shard] = p_send[half, shard]

    def send_prefixes(half):
        def body(step, carry):
            to, dev = peer(step)
            pltpu.make_async_remote_copy(
                p_send.at[half, to], p_recv.at[half, shard], ps.at[half], pr.at[half],
                device_id=dev, device_id_type=MESH,
            ).start()
            return carry
        lax.fori_loop(1, SHARDS, body, 0)

    def retention(s, half):
        row = lax.broadcasted_iota(jnp.int32, (256, 256), 0)
        col = lax.broadcasted_iota(jnp.int32, (256, 256), 1)
        def body(hh, carry):
            h = half * 2 + hh
            p = s * 2 + hh
            before = p_recv[half, pl.ds(p * 4, 4)].reshape(DK, DV)
            for i in range(2):
                q = queries[s, h, pl.ds(i * 256, 256)]
                mixed = jnp.dot(q, before, preferred_element_type=F32)
                for j in range(i + 1):
                    k = keys[s, h, pl.ds(j * 256, 256)]
                    sc = lax.dot_general(q, k, (((1,), (1,)), ((), ())), preferred_element_type=F32)
                    if i == j:
                        sc = jnp.where(row >= col, sc, 0.0)
                    mixed = mixed + jnp.dot(
                        sc.astype(BF16), values[s, h, pl.ds(j * 256, 256)], preferred_element_type=F32
                    )
                mu = jnp.sum(mixed, axis=1, keepdims=True) * (1.0 / DV)
                sq = jnp.sum(mixed * mixed, axis=1, keepdims=True) * (1.0 / DV)
                done = ((mixed - mu) * lax.rsqrt(sq - mu * mu + EPS_GROUP)).astype(BF16)
                rows = pl.ds(i * 256, 256)
                if s == 0:
                    for g in range(2):
                        at = pl.multiple_of((g * HEADS + c * 4 + h) * 128, 128)
                        ret[rows, pl.ds(at, 128)] = done[:, g * 128 : (g + 1) * 128]
                else:
                    ret_send[h, rows] = done
            if s == 1:
                for g in range(2):
                    at = pl.multiple_of((g * HEADS + c * 4 + h) * 128, 128)
                    pltpu.make_async_remote_copy(
                        ret_send.at[h, :, pl.ds(g * 128, 128)], ret.at[:, pl.ds(at, 128)],
                        rs.at[h], rr.at[h], device_id=mate, device_id_type=MESH,
                    ).start()
            return carry
        lax.fori_loop(0, 2, body, 0)

    def out_copy(j, core):
        at = pl.multiple_of(core * 1024 + j * 256, 256)
        slot = j if core is c else j + 4
        return pltpu.make_async_copy(out_v.at[slot], out.at[0, :, pl.ds(at, 256)], out_sem.at[slot])

    def out_piece(core, j):
        slot = j if core is c else j + 4
        if core is not c:
            drain(w.at[0], orr.at[j])
        prod = jnp.dot(ret[...], w[O_FIRST + slot].reshape(D, 256), preferred_element_type=F32)
        out_v[slot] = prod.astype(BF16)
        out_copy(j, core).start()

    def wait_prefixes(half):
        drain(p_recv.at[half, pl.ds(0, SHARDS - 1)], pr.at[half])

    def wait_retained():
        for h in range(4):
            drain(ret_send.at[0], rr.at[h])

    stage_p(0)
    stage_p(1)
    stage_p(2)
    stage_p(3)
    stage_a(0)
    stage_a(2)
    for cp in in_copies:
        cp.wait()
    norm(0)
    stage_a(1)
    norm(1)
    stage_b(0)
    stage_b(2)
    stage_b(1)
    stage_c(0)
    stage_d(0, 0)
    stage_d(0, 1)
    tables()
    norm_copy(0).start()
    stage_c(1)
    norm_copy(1).start()
    stage_e(0, 1)
    rate_copy.start()
    norm(2)
    stage_a(3)
    norm_copy(2).start()
    norm(3)
    norm_copy(3).start()
    stage_f(0, 1)
    stage_d(0, 2)
    stage_d(1, 1)
    stage_e(0, 2)
    stage_d(1, 0)
    stage_d(1, 2)
    rate_copy.wait()
    decays()
    stage_e(0, 0)
    stage_f(0, 0)
    stage_c(2)
    for i in range(4):
        norm_copy(i).wait()
    value_piece(0)
    key_piece(0)
    stage_f(0, 2)
    stage_e(1, 2)
    value_piece(1)
    local_states(0)
    stage_f(1, 2)
    send_states(0)
    value_piece(3)
    stage_e(1, 1)
    stage_e(1, 0)
    stage_d(2, 0)
    stage_f(1, 1)
    value_piece(2)
    stage_f(1, 0)
    key_piece(1)
    stage_b(3)
    local_states(1)
    send_states(1)
    stage_d(2, 1)
    stage_c(3)
    scan_states(0)
    stage_e(2, 1)
    send_prefixes(0)
    stage_e(2, 0)
    stage_f(2, 0)
    scan_states(1)
    send_prefixes(1)
    stage_d(3, 2)
    stage_e(3, 2)
    stage_f(2, 1)
    query_piece(0)
    query_piece(1)
    stage_d(2, 2)
    wait_prefixes(0)
    stage_d(3, 1)
    retention(0, 0)
    stage_e(2, 2)
    stage_d(3, 0)
    retention(1, 0)
    stage_f(3, 2)
    wait_prefixes(1)
    retention(1, 1)
    retention(0, 1)
    stage_e(3, 1)
    stage_f(2, 2)
    stage_f(3, 1)
    wait_retained()
    stage_e(3, 0)
    out_piece(c, 0)
    out_piece(other, 3)
    out_piece(c, 2)
    out_piece(c, 3)
    stage_f(3, 0)
    out_piece(other, 2)
    out_piece(other, 0)
    out_piece(c, 1)
    out_piece(other, 1)

    for wave in range(WAVES):
        finish_sends(wave)
    for half in range(2):
        drain(s_recv.at[half, pl.ds(0, SHARDS - 1)], ss.at[half])
        drain(p_recv.at[half, pl.ds(0, SHARDS - 1)], ps.at[half])
    for h in range(4):
        drain(ret_send.at[0], rs.at[h])
        drain(w.at[0], os.at[h])
    for j in range(4):
        out_copy(j, c).wait()
        out_copy(j, other).wait()


def body(tokens, norm_gain, w_query, w_key, w_value, w_out, decay_rate):
    high, low = rope_constants()
    any_spec = pl.BlockSpec(memory_space=pl.ANY)
    dma = pltpu.SemaphoreType.DMA
    scratch = [
        pltpu.VMEM((16, 4, 4, 4, 32, 256), BF16),
        pltpu.VMEM((12, 16, 256), BF16),
        pltpu.VMEM((LEN, D), BF16),
        pltpu.VMEM((2, LEN, D), BF16),
        pltpu.VMEM((1, D), F32),
        pltpu.VMEM((2, 16, DK), F32),
        pltpu.VMEM((2, 32, DK), F32),
        pltpu.VMEM((HEADS, 64), F32),
        pltpu.VMEM((HEADS, 64), F32),
        pltpu.VMEM((LEN, DK), F32),
        pltpu.VMEM((LEN, DK), F32),
        pltpu.VMEM((2, 4, 4, 128), F32),
        pltpu.VMEM((2, 5, 4, 128), F32),
        pltpu.VMEM((2, 4, SHARDS, 128), F32),
        pltpu.VMEM((2, 4, LEN, DK), BF16),
        pltpu.VMEM((2, 4, LEN, DK), BF16),
        pltpu.VMEM((2, 4, LEN, DV), BF16),
        pltpu.VMEM((2, SHARDS, 32, DV), BF16),
        pltpu.VMEM((2, SHARDS, 32, DV), BF16),
        pltpu.VMEM((2, SHARDS, 32, DV), BF16),
        pltpu.VMEM((2, SHARDS, 32, DV), BF16),
        pltpu.VMEM((LEN, D), BF16),
        pltpu.VMEM((4, LEN, DV), BF16),
        pltpu.VMEM((8, LEN, 256), BF16),
        dma((4,)), dma((4,)), dma((WAVES,)), dma((WAVES,)), dma((WAVES,)), dma, dma, dma((4,)), dma((4,)),
        dma((WAVES,)), dma((WAVES,)), dma((WAVES,)), dma((WAVES,)), dma((WAVES,)), dma((WAVES,)),
        dma((WAVES,)), dma((WAVES, 3, 2, 2)), dma((WAVES, 3)), dma((WAVES, 3, 2)),
        dma((2,)), dma((2,)), dma((2,)), dma((2,)), dma((4,)), dma((4,)), dma((4,)), dma((4,)), dma((8,)),
    ]
    return pl.pallas_call(
        kernel,
        out_shape=jax.ShapeDtypeStruct((1, LEN, D), BF16),
        in_specs=[any_spec] * 9,
        out_specs=any_spec,
        scratch_shapes=scratch,
        compiler_params=pltpu.CompilerParams(
            collective_id=0, has_side_effects=True, vmem_limit_bytes=60 * 1024 * 1024
        ),
    )(tokens, norm_gain[None], w_query, w_key, w_value, w_out, decay_rate[0], jnp.asarray(high), jnp.asarray(low))


def solution(mesh):
    split = Mesh(mesh.devices.reshape(4, 4, 4, 2), ("z", "y", "x", "c"))
    in_specs = (
        P(("x", "c"), ("z", "y"), None),
        P(),
        P(("z", "y", "x", "c"), None),
        P(("z", "y", "x", "c"), None),
        P(("z", "y", "x", "c"), None),
        P(("z", "y", "x", "c"), None),
        P(("x", "c"), None, None),
    )
    return jax.shard_map(
        body, mesh=split, in_specs=in_specs, out_specs=P(("x", "c"), ("z", "y"), None), check_vma=False
    )
```

```python
import functools

import jax
import jax.numpy as jnp
import numpy as np
from jax import lax
from jax.experimental import pallas as pl
from jax.experimental.pallas import tpu as pltpu
from jax.sharding import Mesh
from jax.sharding import PartitionSpec as P

MESH = pl.DeviceIdType.MESH
F32 = jnp.float32
BF16 = jnp.bfloat16

HEADS = 8
DK = 128
DV = 256
BLOCK = 128
D = 2048
LEN = 512
SHARDS = 16
EPS_RMS = 1e-06
EPS_GROUP = 0.01
ROPE_BASE = 10000.0

K_PIECES = (0, 3)
V_PIECES = (1, 2, 4, 5)
Q_PIECES = (6, 7)
O_FIRST = 8
WAVES = 4
ORDERS = (
    ((2, 1, 0), (1, 0, 2), (0, 2, 1)),
    ((2, 1, 0), (1, 0, 2), (0, 2, 1)),
    ((1, 2, 0), (0, 1, 2), (2, 0, 1)),
    ((0, 2, 1), (1, 2, 0), (0, 1, 2)),
)


def rope_constants():
    inverse = ROPE_BASE ** (-(np.arange(DK // 2, dtype=np.float64) / (DK // 2 - 1)))
    inverse = np.repeat(inverse, 2)
    high = np.arange(256, dtype=np.float64)[:, None] * 32 * inverse[None, :]
    low = np.arange(32, dtype=np.float64)[:, None] * inverse[None, :]
    high = np.stack([np.cos(high), np.sin(high)]).astype(np.float32)
    low = np.stack([np.cos(low), np.sin(low)]).astype(np.float32)
    return high, low


def kernel(
    tokens, gain_in, wq, wk, wv, wo, rates_in, high_in, low_in,
    out,
    w, for_mate, x_raw, xn, gain, high, low, rates, rates2, cos_t, sin_t, rate_b, base_b, dec,
    keys, queries, values, s_send, s_recv, p_send, p_recv, ret, ret_send,
    in_sem, tok_sem, own_sem, mate_s, mate_r, rate_s, rate_r, xn_s, xn_r,
    p1s, p1r, p2s, p2r, p2fs, p2fr, p3s, p3r, p3fs, p3fr,
    ss, sr, ps, pr, rs, rr, os, orr,
):
    z, y, x, c = (lax.axis_index(a) for a in ("z", "y", "x", "c"))
    here = (z, y, x)
    shard = z * 4 + y
    mate = (z, y, x, 1 - c)

    def device(dim, step, core=None):
        at = list(here)
        at[dim] = lax.rem(at[dim] + step, 4)
        return (*at, c if core is None else core)

    def peer(step):
        to = lax.rem(shard + step, SHARDS)
        return to, (lax.div(to, 4), lax.rem(to, 4), x, c)

    tok_copies = []
    for i in range(4):
        rows = pl.ds(i * 128, 128)
        cp = pltpu.make_async_copy(tokens.at[0, rows], x_raw.at[rows], tok_sem.at[i])
        tok_copies.append(cp)

    def pieces_of(wave, core):
        todo = []
        for piece in range(3 * wave, 3 * wave + 3):
            if piece in K_PIECES or piece in Q_PIECES:
                ref = wk if piece in K_PIECES else wq
                j = K_PIECES.index(piece) if piece in K_PIECES else Q_PIECES.index(piece)
                at = pl.multiple_of(core * 512 + j * 256, 256)
                todo.append((ref.at[:, pl.ds(at, 256)], piece, pl.ds(0, 256)))
            elif piece in V_PIECES:
                h = V_PIECES.index(piece)
                for s in range(2):
                    at = pl.multiple_of(core * 512 + (s * 1024 + h * 128), 128)
                    todo.append((wv.at[:, pl.ds(at, 128)], piece, pl.ds(s * 128, 128)))
            else:
                at = pl.multiple_of(core * 1024 + (piece - O_FIRST) * 256, 256)
                todo.append((wo.at[:, pl.ds(at, 256)], piece, pl.ds(0, 256)))
        return todo

    own_rows = pl.ds(pl.multiple_of(c * 16, 16), 16)
    other = 1 - c

    barrier = pltpu.get_barrier_semaphore()
    first_peers = [mate]
    for dim in range(3):
        for step in (1, 3, 2):
            first_peers += [device(dim, step), device(dim, step, other)]
    for dev in first_peers:
        pl.semaphore_signal(barrier, inc=1, device_id=dev, device_id_type=MESH)

    in_copies = [
        pltpu.make_async_copy(gain_in, gain, in_sem.at[0]),
        pltpu.make_async_copy(rates_in, rates, in_sem.at[1]),
        pltpu.make_async_copy(high_in.at[:, pl.ds(pl.multiple_of(shard * 16, 16), 16)], high, in_sem.at[2]),
        pltpu.make_async_copy(low_in, low, in_sem.at[3]),
    ]
    for cp in in_copies + tok_copies:
        cp.start()
    for wave in range(WAVES):
        for src, piece, cols in pieces_of(wave, c):
            pltpu.make_async_copy(src, w.at[piece, z, y, x, own_rows, cols], own_sem.at[wave]).start()
        for src, piece, cols in pieces_of(wave, other):
            pltpu.make_async_copy(src, for_mate.at[piece, :, cols], own_sem.at[wave]).start()
    pl.semaphore_wait(barrier, len(first_peers))
    rate_copy = pltpu.make_async_remote_copy(
        rates_in, rates2, rate_s, rate_r, device_id=mate, device_id_type=MESH
    )

    def part_slice(piece, where):
        idx = tuple(where.get(d, pl.ds(0, 4)) for d in range(3))
        return w.at[(piece, *idx)]

    def send(src, ssem, rsem, dev):
        pltpu.make_async_remote_copy(src, src, ssem, rsem, device_id=dev, device_id_type=MESH).start()

    def drain(ref, sem):
        pltpu.make_async_copy(ref, ref, sem).wait()

    def three(wave):
        return pl.ds(3 * wave, 3)

    def p1_wait_ref(wave):
        return w.at[three(wave), 0, 0, pl.ds(0, 3)]

    def p2_wait_ref(wave):
        return w.at[three(wave), pl.ds(0, 2), 0]

    def p2f_wait_ref(wave):
        return w.at[three(wave), 0, 0]

    def half_wait_ref(wave):
        return w.at[3 * wave, pl.ds(0, 2), 0]

    HALF = (pl.ds(0, 2), pl.ds(2, 2))

    def stage_p(wave):
        drain(w.at[three(wave), 0, 0, 0], own_sem.at[wave])
        for part, (d1, d2, d3) in enumerate(ORDERS[wave]):
            piece = 3 * wave + part
            own = w.at[piece, z, y, x, own_rows]
            pltpu.make_async_remote_copy(
                for_mate.at[piece], own, mate_s.at[wave], mate_r.at[wave], device_id=mate, device_id_type=MESH
            ).start()
            for step in (1, 3, 2):
                for src, core in ((own, c), (for_mate.at[piece], other)):
                    pltpu.make_async_remote_copy(
                        src, own, p1s.at[wave], p1r.at[wave],
                        device_id=device(d1, step, core), device_id_type=MESH,
                    ).start()

    def stage_a(wave):
        drain(w.at[three(wave), 0, 0, 0, pl.ds(0, 16)], mate_r.at[wave])
        drain(p1_wait_ref(wave), p1r.at[wave])
        for part, (d1, d2, d3) in enumerate(ORDERS[wave]):
            own = part_slice(3 * wave + part, {d2: here[d2], d3: here[d3]})
            for step in (1, 3):
                send(own, p2s.at[wave], p2r.at[wave], device(d2, step))

    def stage_b(wave):
        drain(p2_wait_ref(wave), p2r.at[wave])
        for part, (d1, d2, d3) in enumerate(ORDERS[wave]):
            for i, step in enumerate((1, 3)):
                origin = lax.rem(here[d2] + 4 - step, 4)
                src = part_slice(3 * wave + part, {d1: HALF[i], d2: origin, d3: here[d3]})
                send(src, p2fs.at[wave], p2fr.at[wave], device(d2, step))

    def stage_c(wave):
        drain(p2f_wait_ref(wave), p2fr.at[wave])
        for sub in range(2):
            for part, (d1, d2, d3) in enumerate(ORDERS[wave]):
                for i, step in enumerate((1, 3)):
                    half = sub if i == 0 else 1 - sub
                    src = part_slice(3 * wave + part, {d2: HALF[half], d3: here[d3]})
                    send(src, p3s.at[wave], p3r.at[wave, part, i, sub], device(d3, step))
        for part in range(3):
            if 3 * wave + part >= O_FIRST:
                d3 = ORDERS[wave][part][2]
                pass_on(3 * wave + part, d3, here[d3])

    def stage_d(wave, part):
        d1, d2, d3 = ORDERS[wave][part]
        for i, step in enumerate((1, 3)):
            drain(half_wait_ref(wave), p3r.at[wave, part, i, 0])
            origin = lax.rem(here[d3] + 4 - step, 4)
            src = part_slice(3 * wave + part, {d2: HALF[i], d3: origin})
            send(src, p3fs.at[wave, part], p3fr.at[wave, part, i], device(d3, step))

    def pass_on(piece, d3, at):
        j = piece - O_FIRST
        pltpu.make_async_remote_copy(
            part_slice(piece, {d3: at}), part_slice(piece + 4, {d3: at}),
            os.at[j], orr.at[j], device_id=mate, device_id_type=MESH,
        ).start()

    def stage_e(wave, part):
        piece = 3 * wave + part
        d3 = ORDERS[wave][part][2]
        for i, step in enumerate((1, 3)):
            drain(half_wait_ref(wave), p3r.at[wave, part, i, 1])
            if piece >= O_FIRST:
                pass_on(piece, d3, lax.rem(here[d3] + 4 - step, 4))

    def stage_f(wave, part):
        piece = 3 * wave + part
        d3 = ORDERS[wave][part][2]
        for i in range(2):
            drain(half_wait_ref(wave), p3fr.at[wave, part, i])
        if piece >= O_FIRST:
            pass_on(piece, d3, lax.rem(here[d3] + 2, 4))

    def finish_sends(wave):
        drain(w.at[three(wave), 0, 0, 0, pl.ds(0, 16)], mate_s.at[wave])
        drain(p1_wait_ref(wave), p1s.at[wave])
        drain(p2_wait_ref(wave), p2s.at[wave])
        drain(p2f_wait_ref(wave), p2fs.at[wave])
        drain(w.at[three(wave), pl.ds(0, 2)], p3s.at[wave])
        for part in range(3):
            drain(w.at[3 * wave, 0], p3fs.at[wave, part])

    def norm(i):
        rows = pl.ds(i * 128, 128)
        tok_copies[i].wait()
        wide = x_raw[rows].astype(F32)
        inv = lax.rsqrt(jnp.sum(wide * wide, axis=-1, keepdims=True) * (1.0 / D) + EPS_RMS)
        xn[0, rows] = (wide * inv * gain[...]).astype(BF16)

    def norm_copy(i):
        rows = pl.ds(i * 128, 128)
        return pltpu.make_async_remote_copy(
            xn.at[0, rows], xn.at[1, rows], xn_s.at[i], xn_r.at[i], device_id=mate, device_id_type=MESH
        )

    def tables():
        lane = lax.broadcasted_iota(jnp.int32, (32, DK), 1)
        sign = jnp.where(lax.rem(lane, 2) == 0, -1.0, 1.0).astype(F32)
        cl, sl = low[0], low[1]
        for i in range(16):
            ch, sh = high[0, pl.ds(i, 1)], high[1, pl.ds(i, 1)]
            cos_t[pl.ds(i * 32, 32)] = ch * cl - sh * sl
            sin_t[pl.ds(i * 32, 32)] = (sh * cl + ch * sl) * sign

    def decays():
        lane = lax.broadcasted_iota(jnp.int32, (4, 64), 1)
        for s in range(2):
            full = rates[...] if s == 0 else rates2[...]
            mine = jnp.where(c == 0, full[0:4], full[4:8])
            base = jnp.zeros((4, 1), F32)
            for n in range(4):
                r = jnp.sum(jnp.where(lane == shard * 4 + n, mine, 0.0), axis=1, keepdims=True)
                rate_b[s, n] = jnp.broadcast_to(r, (4, 128))
                base_b[s, n] = jnp.broadcast_to(base, (4, 128))
                base = base + r * float(BLOCK)
            base_b[s, 4] = jnp.broadcast_to(base, (4, 128))
            for t in range(SHARDS - 1):
                tot = jnp.sum(jnp.where(lax.div(lane, 4) == t, mine, 0.0), axis=1, keepdims=True)
                e = jnp.broadcast_to(jnp.exp(tot * (-float(BLOCK))), (4, 128))
                for h in range(4):
                    dec[h // 2, s * 2 + h % 2, pl.ds(t, 1)] = e[h : h + 1]

    def turned(prod, s, h, sign, scale):
        v = prod.astype(BF16).astype(F32)
        even = lax.rem(lax.broadcasted_iota(jnp.int32, v.shape, 1), 2) == 0
        swap = jnp.where(even, pltpu.roll(v, DK - 1, 1), pltpu.roll(v, 1, 1))
        rot = v * cos_t[...] + swap * sin_t[...]
        offset = (lax.broadcasted_iota(jnp.int32, (BLOCK, DK), 0) + 1).astype(F32)
        parts = []
        for n in range(4):
            e = base_b[s, n, pl.ds(h, 1)] + rate_b[s, n, pl.ds(h, 1)] * offset
            parts.append(rot[n * BLOCK : (n + 1) * BLOCK] * (jnp.exp(e * sign) * scale))
        return jnp.concatenate(parts, axis=0).astype(BF16)

    def project(piece):
        return jnp.dot(
            xn[...].reshape(2 * LEN, D), w[piece].reshape(D, 256), preferred_element_type=F32
        ).reshape(2, LEN, 256)

    def key_piece(j):
        prod = project(K_PIECES[j])
        for s in range(2):
            for hh in range(2):
                h = 2 * j + hh
                keys[s, h] = turned(prod[s, :, hh * 128 : (hh + 1) * 128], s, h, 1.0, DK ** (-0.5))

    def query_piece(j):
        prod = project(Q_PIECES[j])
        for s in range(2):
            for hh in range(2):
                h = 2 * j + hh
                queries[s, h] = turned(prod[s, :, hh * 128 : (hh + 1) * 128], s, h, -1.0, 1.0)

    def value_piece(h):
        prod = project(V_PIECES[h])
        for s in range(2):
            values[s, h] = prod[s].astype(BF16)

    def local_states(half):
        for p in range(4):
            s, h = p // 2, half * 2 + p % 2
            st = lax.dot_general(
                keys[s, h], values[s, h], (((0,), (0,)), ((), ())), preferred_element_type=F32
            )
            e = jnp.exp(-base_b[s, 4, pl.ds(h, 1)])
            e = jnp.concatenate([e, e], axis=1)
            s_send[half, pl.ds(p * 4, 4)] = (st * e).astype(BF16).reshape(4, 32, DV)
        s_recv[half, shard] = s_send[half, shard]

    def send_states(half):
        def body(step, carry):
            to, dev = peer(step)
            pltpu.make_async_remote_copy(
                s_send.at[half, to], s_recv.at[half, shard], ss.at[half], sr.at[half],
                device_id=dev, device_id_type=MESH,
            ).start()
            return carry
        lax.fori_loop(1, SHARDS, body, 0)

    def scan_states(half):
        drain(s_recv.at[half, pl.ds(0, SHARDS - 1)], sr.at[half])
        run = jnp.zeros((32, DV), F32)
        rows = dec[half, z]
        for t in range(SHARDS):
            p_send[half, t] = run.astype(BF16)
            if t < SHARDS - 1:
                e = rows[t : t + 1]
                run = run * jnp.concatenate([e, e], axis=1) + s_recv[half, t].astype(F32)
        p_recv[half, shard] = p_send[half, shard]

    def send_prefixes(half):
        def body(step, carry):
            to, dev = peer(step)
            pltpu.make_async_remote_copy(
                p_send.at[half, to], p_recv.at[half, shard], ps.at[half], pr.at[half],
                device_id=dev, device_id_type=MESH,
            ).start()
            return carry
        lax.fori_loop(1, SHARDS, body, 0)

    def retention(s, half):
        row = lax.broadcasted_iota(jnp.int32, (256, 256), 0)
        col = lax.broadcasted_iota(jnp.int32, (256, 256), 1)
        for hh in range(2):
            h = half * 2 + hh
            p = s * 2 + hh
            before = p_recv[half, pl.ds(p * 4, 4)].reshape(DK, DV)
            for i in range(2):
                q = queries[s, h, pl.ds(i * 256, 256)]
                mixed = jnp.dot(q, before, preferred_element_type=F32)
                for j in range(i + 1):
                    k = keys[s, h, pl.ds(j * 256, 256)]
                    sc = lax.dot_general(q, k, (((1,), (1,)), ((), ())), preferred_element_type=F32)
                    if i == j:
                        sc = jnp.where(row >= col, sc, 0.0)
                    mixed = mixed + jnp.dot(
                        sc.astype(BF16), values[s, h, pl.ds(j * 256, 256)], preferred_element_type=F32
                    )
                mu = jnp.sum(mixed, axis=1, keepdims=True) * (1.0 / DV)
                sq = jnp.sum(mixed * mixed, axis=1, keepdims=True) * (1.0 / DV)
                done = ((mixed - mu) * lax.rsqrt(sq - mu * mu + EPS_GROUP)).astype(BF16)
                rows = pl.ds(i * 256, 256)
                if s == 0:
                    for g in range(2):
                        at = pl.multiple_of((g * HEADS + c * 4 + h) * 128, 128)
                        ret[rows, pl.ds(at, 128)] = done[:, g * 128 : (g + 1) * 128]
                else:
                    ret_send[h, rows] = done
            if s == 1:
                for g in range(2):
                    at = pl.multiple_of((g * HEADS + c * 4 + h) * 128, 128)
                    pltpu.make_async_remote_copy(
                        ret_send.at[h, :, pl.ds(g * 128, 128)], ret.at[:, pl.ds(at, 128)],
                        rs.at[h], rr.at[h], device_id=mate, device_id_type=MESH,
                    ).start()

    def out_piece(core, j):
        slot = j if core is c else j + 4
        if core is not c:
            drain(w.at[0], orr.at[j])
        prod = jnp.dot(ret[...], w[O_FIRST + slot].reshape(D, 256), preferred_element_type=F32)
        at = pl.multiple_of(core * 1024 + j * 256, 256)
        out[0, :, pl.ds(at, 256)] = prod.astype(BF16)

    def wait_prefixes(half):
        drain(p_recv.at[half, pl.ds(0, SHARDS - 1)], pr.at[half])

    def wait_retained():
        for h in range(4):
            drain(ret_send.at[0], rr.at[h])

    def block(step, *args):
        pl.when(z < 4)(functools.partial(step, *args))

    stage_p(0)
    stage_p(1)
    stage_p(2)
    stage_p(3)
    stage_a(0)
    stage_a(2)
    for cp in in_copies:
        cp.wait()
    block(norm, 0)
    stage_a(1)
    block(norm, 1)
    stage_b(0)
    stage_b(2)
    stage_b(1)
    stage_c(0)
    stage_d(0, 0)
    stage_d(0, 1)
    block(tables)
    norm_copy(0).start()
    stage_c(1)
    norm_copy(1).start()
    stage_e(0, 1)
    rate_copy.start()
    block(norm, 2)
    stage_a(3)
    norm_copy(2).start()
    block(norm, 3)
    norm_copy(3).start()
    stage_f(0, 1)
    stage_d(0, 2)
    stage_d(1, 1)
    stage_e(0, 2)
    stage_d(1, 0)
    stage_d(1, 2)
    rate_copy.wait()
    block(decays)
    stage_e(0, 0)
    stage_f(0, 0)
    stage_c(2)
    for i in range(4):
        norm_copy(i).wait()
    block(value_piece, 0)
    block(key_piece, 0)
    stage_f(0, 2)
    stage_e(1, 2)
    block(value_piece, 1)
    block(local_states, 0)
    stage_f(1, 2)
    send_states(0)
    block(value_piece, 3)
    stage_e(1, 1)
    stage_e(1, 0)
    stage_d(2, 0)
    stage_f(1, 1)
    block(value_piece, 2)
    stage_f(1, 0)
    block(key_piece, 1)
    stage_b(3)
    block(local_states, 1)
    send_states(1)
    stage_d(2, 1)
    stage_c(3)
    block(scan_states, 0)
    stage_e(2, 1)
    send_prefixes(0)
    stage_e(2, 0)
    stage_f(2, 0)
    block(scan_states, 1)
    send_prefixes(1)
    stage_d(3, 2)
    stage_e(3, 2)
    stage_f(2, 1)
    block(query_piece, 0)
    block(query_piece, 1)
    stage_d(2, 2)
    wait_prefixes(0)
    stage_d(3, 1)
    block(retention, 0, 0)
    stage_e(2, 2)
    stage_d(3, 0)
    block(retention, 1, 0)
    stage_f(3, 2)
    wait_prefixes(1)
    block(retention, 1, 1)
    block(retention, 0, 1)
    stage_e(3, 1)
    stage_f(2, 2)
    stage_f(3, 1)
    wait_retained()
    stage_e(3, 0)
    block(out_piece, c, 0)
    block(out_piece, other, 3)
    block(out_piece, c, 2)
    block(out_piece, c, 3)
    stage_f(3, 0)
    block(out_piece, other, 2)
    block(out_piece, other, 0)
    block(out_piece, c, 1)
    block(out_piece, other, 1)

    for wave in range(WAVES):
        finish_sends(wave)
    for half in range(2):
        drain(s_recv.at[half, pl.ds(0, SHARDS - 1)], ss.at[half])
        drain(p_recv.at[half, pl.ds(0, SHARDS - 1)], ps.at[half])
    for h in range(4):
        drain(ret_send.at[0], rs.at[h])
        drain(w.at[0], os.at[h])


def body(tokens, norm_gain, w_query, w_key, w_value, w_out, decay_rate):
    high, low = rope_constants()
    any_spec = pl.BlockSpec(memory_space=pl.ANY)
    dma = pltpu.SemaphoreType.DMA
    scratch = [
        pltpu.VMEM((16, 4, 4, 4, 32, 256), BF16),
        pltpu.VMEM((12, 16, 256), BF16),
        pltpu.VMEM((LEN, D), BF16),
        pltpu.VMEM((2, LEN, D), BF16),
        pltpu.VMEM((1, D), F32),
        pltpu.VMEM((2, 16, DK), F32),
        pltpu.VMEM((2, 32, DK), F32),
        pltpu.VMEM((HEADS, 64), F32),
        pltpu.VMEM((HEADS, 64), F32),
        pltpu.VMEM((LEN, DK), F32),
        pltpu.VMEM((LEN, DK), F32),
        pltpu.VMEM((2, 4, 4, 128), F32),
        pltpu.VMEM((2, 5, 4, 128), F32),
        pltpu.VMEM((2, 4, SHARDS, 128), F32),
        pltpu.VMEM((2, 4, LEN, DK), BF16),
        pltpu.VMEM((2, 4, LEN, DK), BF16),
        pltpu.VMEM((2, 4, LEN, DV), BF16),
        pltpu.VMEM((2, SHARDS, 32, DV), BF16),
        pltpu.VMEM((2, SHARDS, 32, DV), BF16),
        pltpu.VMEM((2, SHARDS, 32, DV), BF16),
        pltpu.VMEM((2, SHARDS, 32, DV), BF16),
        pltpu.VMEM((LEN, D), BF16),
        pltpu.VMEM((4, LEN, DV), BF16),
        dma((4,)), dma((4,)), dma((WAVES,)), dma((WAVES,)), dma((WAVES,)), dma, dma, dma((4,)), dma((4,)),
        dma((WAVES,)), dma((WAVES,)), dma((WAVES,)), dma((WAVES,)), dma((WAVES,)), dma((WAVES,)),
        dma((WAVES,)), dma((WAVES, 3, 2, 2)), dma((WAVES, 3)), dma((WAVES, 3, 2)),
        dma((2,)), dma((2,)), dma((2,)), dma((2,)), dma((4,)), dma((4,)), dma((4,)), dma((4,)),
    ]
    args = (
        tokens, norm_gain[None], w_query, w_key, w_value, w_out, decay_rate[0],
        jnp.asarray(high), jnp.asarray(low),
    )
    return pl.pallas_call(
        kernel,
        out_shape=jax.ShapeDtypeStruct((1, LEN, D), BF16),
        in_specs=[any_spec] * 9,
        out_specs=pl.BlockSpec(memory_space=pltpu.VMEM),
        scratch_shapes=scratch,
        compiler_params=pltpu.CompilerParams(
            collective_id=0, has_side_effects=True, vmem_limit_bytes=44 * 1024 * 1024
        ),
    )(*(pltpu.with_memory_space_constraint(a, pltpu.HBM) for a in args))


def solution(mesh):
    split = Mesh(mesh.devices.reshape(4, 4, 4, 2), ("z", "y", "x", "c"))
    in_specs = (
        P(("x", "c"), ("z", "y"), None),
        P(),
        P(("z", "y", "x", "c"), None),
        P(("z", "y", "x", "c"), None),
        P(("z", "y", "x", "c"), None),
        P(("z", "y", "x", "c"), None),
        P(("x", "c"), None, None),
    )
    return jax.shard_map(
        body, mesh=split, in_specs=in_specs, out_specs=P(("x", "c"), ("z", "y"), None), check_vma=False
    )
```

```python
import functools

import jax
import jax.numpy as jnp
import numpy as np
from jax import lax
from jax.experimental import pallas as pl
from jax.experimental.pallas import tpu as pltpu
from jax.sharding import Mesh
from jax.sharding import PartitionSpec as P

MESH = pl.DeviceIdType.MESH
F32 = jnp.float32
BF16 = jnp.bfloat16

HEADS = 8
DK = 128
DV = 256
BLOCK = 128
D = 2048
LEN = 512
SHARDS = 16
EPS_RMS = 1e-06
EPS_GROUP = 0.01
ROPE_BASE = 10000.0

PLAN = (
    (((1, 2, 0), "Q"), ((0, 1, 2), "K"), ((2, 0, 1), "V")),
    (((2, 1, 0), "KV"), ((1, 0, 2), "VVV"), ((0, 2, 1), "KKV")),
    (((2, 1, 0), "VV"), ((0, 2, 1), "Q"), ((1, 0, 2), "QQOO")),
    (((2, 0, 1), "OO"), ((2, 1, 0), "O"), ((2, 1, 0), "O")),
    (((0, 1, 2), "OO"), ((0, 2, 1), ""), ((2, 0, 1), "")),
)
WAVES = len(PLAN)
PIECES = 24
KINDS = "".join(kinds for wave in PLAN for _, kinds in wave)


def ranges():
    at, parts, whole = 0, [], []
    for wave in PLAN:
        first, mine = at, []
        for order, kinds in wave:
            mine.append((order, at, len(kinds)))
            at += len(kinds)
        parts.append(mine)
        whole.append((first, at - first))
    return parts, whole


PARTS, WHOLE = ranges()
AT = {kind: [i for i, k in enumerate(KINDS) if k == kind] for kind in "KVQO"}


def rope_constants():
    inverse = ROPE_BASE ** (-(np.arange(DK // 2, dtype=np.float64) / (DK // 2 - 1)))
    inverse = np.repeat(inverse, 2)
    high = np.arange(256, dtype=np.float64)[:, None] * 32 * inverse[None, :]
    low = np.arange(32, dtype=np.float64)[:, None] * inverse[None, :]
    high = np.stack([np.cos(high), np.sin(high)]).astype(np.float32)
    low = np.stack([np.cos(low), np.sin(low)]).astype(np.float32)
    return high, low


def kernel(
    tokens, gain_in, wq, wk, wv, wo, rates_in, high_in, low_in,
    out,
    w, for_mate, x_raw, xn, gain, high, low, rates, rates2, cos_t, sin_t, rate_b, base_b, dec,
    keys, queries, values, s_send, s_recv, p_send, p_recv, ret, ret_send,
    in_sem, tok_sem, own_sem, mate_s, mate_r, rate_s, rate_r, xn_s, xn_r,
    p1s, p1r, p2s, p2r, p2fs, p2fr, p3s, p3r, p3fs, p3fr,
    ss, sr, ps, pr, rs, rr, os, orr,
):
    z, y, x, c = (lax.axis_index(a) for a in ("z", "y", "x", "c"))
    here = (z, y, x)
    shard = z * 4 + y
    mate = (z, y, x, 1 - c)

    def device(dim, step, core=None):
        at = list(here)
        at[dim] = lax.rem(at[dim] + step, 4)
        return (*at, c if core is None else core)

    def peer(step):
        to = lax.rem(shard + step, SHARDS)
        return to, (lax.div(to, 4), lax.rem(to, 4), x, c)

    tok_copies = []
    for i in range(4):
        rows = pl.ds(i * 128, 128)
        cp = pltpu.make_async_copy(tokens.at[0, rows], x_raw.at[rows], tok_sem.at[i])
        tok_copies.append(cp)

    def columns_of(piece, core):
        kind = KINDS[piece]
        i = AT[kind].index(piece)
        if kind == "V":
            ref, at = wv, core * 512 + (i % 2 * 1024 + i // 2 * 128)
        elif kind == "O":
            ref, at = wo, core * 1024 + i * 128
        else:
            ref, at = wk if kind == "K" else wq, core * 512 + i * 128
        return ref.at[:, pl.ds(pl.multiple_of(at, 128), 128)]

    own_rows = pl.ds(pl.multiple_of(c * 16, 16), 16)
    other = 1 - c

    barrier = pltpu.get_barrier_semaphore()
    first_peers = [mate]
    for dim in range(3):
        for step in (1, 3, 2):
            first_peers += [device(dim, step), device(dim, step, other)]
    for dev in first_peers:
        pl.semaphore_signal(barrier, inc=1, device_id=dev, device_id_type=MESH)

    in_copies = [
        pltpu.make_async_copy(gain_in, gain, in_sem.at[0]),
        pltpu.make_async_copy(rates_in, rates, in_sem.at[1]),
        pltpu.make_async_copy(high_in.at[:, pl.ds(pl.multiple_of(shard * 16, 16), 16)], high, in_sem.at[2]),
        pltpu.make_async_copy(low_in, low, in_sem.at[3]),
    ]
    for cp in in_copies + tok_copies:
        cp.start()
    for wave, (first, count) in enumerate(WHOLE):
        for piece in range(first, first + count):
            pltpu.make_async_copy(columns_of(piece, c), w.at[piece, z, y, x, own_rows], own_sem.at[wave]).start()
            pltpu.make_async_copy(columns_of(piece, other), for_mate.at[piece], own_sem.at[wave]).start()
    pl.semaphore_wait(barrier, len(first_peers))
    rate_copy = pltpu.make_async_remote_copy(
        rates_in, rates2, rate_s, rate_r, device_id=mate, device_id_type=MESH
    )

    def part_slice(first, count, where):
        return w.at[(pl.ds(first, count), *(where.get(d, pl.ds(0, 4)) for d in range(3)))]

    def send(src, ssem, rsem, dev):
        pltpu.make_async_remote_copy(src, src, ssem, rsem, device_id=dev, device_id_type=MESH).start()

    def drain(ref, sem):
        pltpu.make_async_copy(ref, ref, sem).wait()

    def rows_of(wave):
        return pl.ds(*WHOLE[wave])

    def p1_wait_ref(wave):
        return w.at[rows_of(wave), 0, 0, pl.ds(0, 3)]

    def p2_wait_ref(wave):
        return w.at[rows_of(wave), pl.ds(0, 2), 0]

    def p2f_wait_ref(wave):
        return w.at[rows_of(wave), 0, 0]

    def mate_wait_ref(wave):
        return w.at[rows_of(wave), 0, 0, 0, pl.ds(0, 16)]

    def half_wait_ref(count):
        return w.at[pl.ds(0, count), pl.ds(0, 2), 0]

    HALF = (pl.ds(0, 2), pl.ds(2, 2))

    def parts_of(wave):
        return [(part, *it) for part, it in enumerate(PARTS[wave]) if it[2]]

    def stage_p(wave):
        drain(w.at[rows_of(wave), 0, 0, 0], own_sem.at[wave])
        for part, (d1, d2, d3), first, count in parts_of(wave):
            pieces = pl.ds(first, count)
            own = w.at[pieces, z, y, x, own_rows]
            theirs = for_mate.at[pieces]
            pltpu.make_async_remote_copy(
                theirs, own, mate_s.at[wave], mate_r.at[wave], device_id=mate, device_id_type=MESH
            ).start()
            for step in (1, 3, 2):
                for src, core in ((own, c), (theirs, other)):
                    pltpu.make_async_remote_copy(
                        src, own, p1s.at[wave], p1r.at[wave],
                        device_id=device(d1, step, core), device_id_type=MESH,
                    ).start()

    def stage_a(wave):
        drain(mate_wait_ref(wave), mate_r.at[wave])
        drain(p1_wait_ref(wave), p1r.at[wave])
        for part, (d1, d2, d3), first, count in parts_of(wave):
            own = part_slice(first, count, {d2: here[d2], d3: here[d3]})
            for step in (1, 3):
                send(own, p2s.at[wave], p2r.at[wave], device(d2, step))

    def stage_b(wave):
        drain(p2_wait_ref(wave), p2r.at[wave])
        for part, (d1, d2, d3), first, count in parts_of(wave):
            for i, step in enumerate((1, 3)):
                origin = lax.rem(here[d2] + 4 - step, 4)
                src = part_slice(first, count, {d1: HALF[i], d2: origin, d3: here[d3]})
                send(src, p2fs.at[wave], p2fr.at[wave], device(d2, step))

    def stage_c(wave):
        drain(p2f_wait_ref(wave), p2fr.at[wave])
        for sub in range(2):
            for part, (d1, d2, d3), first, count in parts_of(wave):
                for i, step in enumerate((1, 3)):
                    half = sub if i == 0 else 1 - sub
                    src = part_slice(first, count, {d2: HALF[half], d3: here[d3]})
                    send(src, p3s.at[wave], p3r.at[wave, part, i, sub], device(d3, step))
        for part, (d1, d2, d3), first, count in parts_of(wave):
            pass_on(first, count, d3, here[d3])

    def stage_d(wave, part):
        (d1, d2, d3), first, count = PARTS[wave][part]
        for i, step in enumerate((1, 3)):
            drain(half_wait_ref(count), p3r.at[wave, part, i, 0])
            origin = lax.rem(here[d3] + 4 - step, 4)
            src = part_slice(first, count, {d2: HALF[i], d3: origin})
            send(src, p3fs.at[wave, part], p3fr.at[wave, part, i], device(d3, step))

    def pass_on(first, count, d3, at):
        for piece in range(first, first + count):
            if KINDS[piece] == "O":
                j = AT["O"].index(piece)
                pltpu.make_async_remote_copy(
                    part_slice(piece, 1, {d3: at}), part_slice(PIECES + j, 1, {d3: at}),
                    os.at[j], orr.at[j], device_id=mate, device_id_type=MESH,
                ).start()

    def stage_e(wave, part):
        (d1, d2, d3), first, count = PARTS[wave][part]
        for i, step in enumerate((1, 3)):
            drain(half_wait_ref(count), p3r.at[wave, part, i, 1])
            pass_on(first, count, d3, lax.rem(here[d3] + 4 - step, 4))

    def stage_f(wave, part):
        (d1, d2, d3), first, count = PARTS[wave][part]
        for i in range(2):
            drain(half_wait_ref(count), p3fr.at[wave, part, i])
        pass_on(first, count, d3, lax.rem(here[d3] + 2, 4))

    def finish_sends(wave):
        drain(mate_wait_ref(wave), mate_s.at[wave])
        drain(p1_wait_ref(wave), p1s.at[wave])
        drain(p2_wait_ref(wave), p2s.at[wave])
        drain(p2f_wait_ref(wave), p2fs.at[wave])
        drain(w.at[rows_of(wave), pl.ds(0, 2)], p3s.at[wave])
        for part, order, first, count in parts_of(wave):
            drain(w.at[pl.ds(first, count), 0], p3fs.at[wave, part])

    def norm(i):
        rows = pl.ds(i * 128, 128)
        tok_copies[i].wait()
        wide = x_raw[rows].astype(F32)
        inv = lax.rsqrt(jnp.sum(wide * wide, axis=-1, keepdims=True) * (1.0 / D) + EPS_RMS)
        xn[0, rows] = (wide * inv * gain[...]).astype(BF16)

    def norm_copy(i):
        rows = pl.ds(i * 128, 128)
        return pltpu.make_async_remote_copy(
            xn.at[0, rows], xn.at[1, rows], xn_s.at[i], xn_r.at[i], device_id=mate, device_id_type=MESH
        )

    def tables():
        lane = lax.broadcasted_iota(jnp.int32, (32, DK), 1)
        sign = jnp.where(lax.rem(lane, 2) == 0, -1.0, 1.0).astype(F32)
        cl, sl = low[0], low[1]
        for i in range(16):
            ch, sh = high[0, pl.ds(i, 1)], high[1, pl.ds(i, 1)]
            cos_t[pl.ds(i * 32, 32)] = ch * cl - sh * sl
            sin_t[pl.ds(i * 32, 32)] = (sh * cl + ch * sl) * sign

    def decays():
        lane = lax.broadcasted_iota(jnp.int32, (4, 64), 1)
        for s in range(2):
            full = rates[...] if s == 0 else rates2[...]
            mine = jnp.where(c == 0, full[0:4], full[4:8])
            base = jnp.zeros((4, 1), F32)
            for n in range(4):
                r = jnp.sum(jnp.where(lane == shard * 4 + n, mine, 0.0), axis=1, keepdims=True)
                rate_b[s, n] = jnp.broadcast_to(r, (4, 128))
                base_b[s, n] = jnp.broadcast_to(base, (4, 128))
                base = base + r * float(BLOCK)
            base_b[s, 4] = jnp.broadcast_to(base, (4, 128))
            for t in range(SHARDS - 1):
                tot = jnp.sum(jnp.where(lax.div(lane, 4) == t, mine, 0.0), axis=1, keepdims=True)
                e = jnp.broadcast_to(jnp.exp(tot * (-float(BLOCK))), (4, 128))
                for h in range(4):
                    dec[h // 2, s * 2 + h % 2, pl.ds(t, 1)] = e[h : h + 1]

    def turned(prod, s, h, sign, scale):
        v = prod.astype(BF16).astype(F32)
        even = lax.rem(lax.broadcasted_iota(jnp.int32, v.shape, 1), 2) == 0
        swap = jnp.where(even, pltpu.roll(v, DK - 1, 1), pltpu.roll(v, 1, 1))
        rot = v * cos_t[...] + swap * sin_t[...]
        offset = (lax.broadcasted_iota(jnp.int32, (BLOCK, DK), 0) + 1).astype(F32)
        parts = []
        for n in range(4):
            e = base_b[s, n, pl.ds(h, 1)] + rate_b[s, n, pl.ds(h, 1)] * offset
            parts.append(rot[n * BLOCK : (n + 1) * BLOCK] * (jnp.exp(e * sign) * scale))
        return jnp.concatenate(parts, axis=0).astype(BF16)

    def pair(pieces):
        return jnp.concatenate([w[piece].reshape(D, 128) for piece in pieces], axis=1)

    def project(kind, j):
        return jnp.dot(
            xn[...].reshape(2 * LEN, D), pair(AT[kind][2 * j : 2 * j + 2]), preferred_element_type=F32
        ).reshape(2, LEN, 256)

    def key_piece(j):
        prod = project("K", j)
        for s in range(2):
            for hh in range(2):
                h = 2 * j + hh
                keys[s, h] = turned(prod[s, :, hh * 128 : (hh + 1) * 128], s, h, 1.0, DK ** (-0.5))

    def query_piece(j):
        prod = project("Q", j)
        for s in range(2):
            for hh in range(2):
                h = 2 * j + hh
                queries[s, h] = turned(prod[s, :, hh * 128 : (hh + 1) * 128], s, h, -1.0, 1.0)

    def value_piece(h):
        prod = project("V", h)
        for s in range(2):
            values[s, h] = prod[s].astype(BF16)

    def local_states(half):
        for p in range(4):
            s, h = p // 2, half * 2 + p % 2
            st = lax.dot_general(
                keys[s, h], values[s, h], (((0,), (0,)), ((), ())), preferred_element_type=F32
            )
            e = jnp.exp(-base_b[s, 4, pl.ds(h, 1)])
            e = jnp.concatenate([e, e], axis=1)
            s_send[half, pl.ds(p * 4, 4)] = (st * e).astype(BF16).reshape(4, 32, DV)
        s_recv[half, shard] = s_send[half, shard]

    def send_states(half):
        def body(step, carry):
            to, dev = peer(step)
            pltpu.make_async_remote_copy(
                s_send.at[half, to], s_recv.at[half, shard], ss.at[half], sr.at[half],
                device_id=dev, device_id_type=MESH,
            ).start()
            return carry
        lax.fori_loop(1, SHARDS, body, 0)

    def scan_states(half):
        drain(s_recv.at[half, pl.ds(0, SHARDS - 1)], sr.at[half])
        run = jnp.zeros((32, DV), F32)
        rows = dec[half, z]
        for t in range(SHARDS):
            p_send[half, t] = run.astype(BF16)
            if t < SHARDS - 1:
                e = rows[t : t + 1]
                run = run * jnp.concatenate([e, e], axis=1) + s_recv[half, t].astype(F32)
        p_recv[half, shard] = p_send[half, shard]

    def send_prefixes(half):
        def body(step, carry):
            to, dev = peer(step)
            pltpu.make_async_remote_copy(
                p_send.at[half, to], p_recv.at[half, shard], ps.at[half], pr.at[half],
                device_id=dev, device_id_type=MESH,
            ).start()
            return carry
        lax.fori_loop(1, SHARDS, body, 0)

    def retention(s, half):
        row = lax.broadcasted_iota(jnp.int32, (256, 256), 0)
        col = lax.broadcasted_iota(jnp.int32, (256, 256), 1)
        for hh in range(2):
            h = half * 2 + hh
            p = s * 2 + hh
            before = p_recv[half, pl.ds(p * 4, 4)].reshape(DK, DV)
            for i in range(2):
                q = queries[s, h, pl.ds(i * 256, 256)]
                mixed = jnp.dot(q, before, preferred_element_type=F32)
                for j in range(i + 1):
                    k = keys[s, h, pl.ds(j * 256, 256)]
                    sc = lax.dot_general(q, k, (((1,), (1,)), ((), ())), preferred_element_type=F32)
                    if i == j:
                        sc = jnp.where(row >= col, sc, 0.0)
                    mixed = mixed + jnp.dot(
                        sc.astype(BF16), values[s, h, pl.ds(j * 256, 256)], preferred_element_type=F32
                    )
                mu = jnp.sum(mixed, axis=1, keepdims=True) * (1.0 / DV)
                sq = jnp.sum(mixed * mixed, axis=1, keepdims=True) * (1.0 / DV)
                done = ((mixed - mu) * lax.rsqrt(sq - mu * mu + EPS_GROUP)).astype(BF16)
                rows = pl.ds(i * 256, 256)
                if s == 0:
                    for g in range(2):
                        at = pl.multiple_of((g * HEADS + c * 4 + h) * 128, 128)
                        ret[rows, pl.ds(at, 128)] = done[:, g * 128 : (g + 1) * 128]
                else:
                    ret_send[h, rows] = done
            if s == 1:
                for g in range(2):
                    at = pl.multiple_of((g * HEADS + c * 4 + h) * 128, 128)
                    pltpu.make_async_remote_copy(
                        ret_send.at[h, :, pl.ds(g * 128, 128)], ret.at[:, pl.ds(at, 128)],
                        rs.at[h], rr.at[h], device_id=mate, device_id_type=MESH,
                    ).start()

    def out_piece(core, j):
        pieces = (2 * j, 2 * j + 1)
        if core is c:
            pieces = [AT["O"][i] for i in pieces]
        else:
            for i in pieces:
                drain(w.at[0], orr.at[i])
            pieces = [PIECES + i for i in pieces]
        prod = jnp.dot(ret[...], pair(pieces), preferred_element_type=F32)
        at = pl.multiple_of(core * 1024 + j * 256, 256)
        out[0, :, pl.ds(at, 256)] = prod.astype(BF16)

    def wait_prefixes(half):
        drain(p_recv.at[half, pl.ds(0, SHARDS - 1)], pr.at[half])

    def wait_retained():
        for h in range(4):
            drain(ret_send.at[0], rr.at[h])

    def wait_inputs():
        for cp in in_copies:
            cp.wait()

    def send_rates():
        rate_copy.start()

    def wait_rates():
        rate_copy.wait()

    def send_normed(i):
        norm_copy(i).start()

    def wait_normed():
        for i in range(4):
            norm_copy(i).wait()

    compute = (
        norm, tables, decays, key_piece, query_piece, value_piece,
        local_states, scan_states, retention, out_piece,
    )

    def run(step, *args):
        with jax.named_scope(step.__name__ + "".join(f"_{a}" for a in args if isinstance(a, int))):
            if step in compute:
                pl.when(z < 4)(functools.partial(step, *args))
            else:
                step(*args)

    run(stage_p, 0)
    run(stage_p, 1)
    run(stage_p, 2)
    run(stage_p, 3)
    run(send_rates)
    run(stage_p, 4)
    run(wait_inputs)
    run(norm, 0)
    run(stage_a, 0)
    run(stage_a, 1)
    run(stage_b, 0)
    run(stage_a, 2)
    run(stage_b, 1)
    run(stage_c, 0)
    run(norm, 1)
    run(stage_a, 4)
    run(stage_b, 2)
    run(stage_c, 1)
    run(stage_d, 1, 0)
    run(norm, 2)
    run(tables)
    run(norm, 3)
    run(send_normed, 3)
    run(send_normed, 0)
    run(stage_d, 0, 2)
    run(stage_d, 0, 1)
    run(wait_rates)
    run(decays)
    run(send_normed, 1)
    run(stage_e, 0, 2)
    run(stage_e, 1, 0)
    run(stage_d, 1, 1)
    run(stage_d, 1, 2)
    run(stage_c, 2)
    run(send_normed, 2)
    run(wait_normed)
    run(stage_f, 0, 2)
    run(stage_e, 1, 1)
    run(stage_f, 1, 0)
    run(stage_b, 4)
    run(stage_e, 0, 1)
    run(stage_f, 0, 1)
    run(stage_e, 1, 2)
    run(key_piece, 0)
    run(stage_d, 2, 0)
    run(stage_d, 0, 0)
    run(value_piece, 0)
    run(stage_f, 1, 1)
    run(value_piece, 1)
    run(local_states, 0)
    run(stage_f, 1, 2)
    run(stage_e, 2, 0)
    run(send_states, 0)
    run(key_piece, 1)
    run(value_piece, 2)
    run(stage_a, 3)
    run(stage_f, 2, 0)
    run(value_piece, 3)
    run(stage_d, 2, 2)
    run(local_states, 1)
    run(send_states, 1)
    run(stage_d, 2, 1)
    run(stage_c, 4)
    run(scan_states, 0)
    run(stage_e, 0, 0)
    run(stage_b, 3)
    run(send_prefixes, 0)
    run(stage_e, 2, 1)
    run(scan_states, 1)
    run(stage_e, 2, 2)
    run(stage_f, 0, 0)
    run(stage_f, 2, 1)
    run(send_prefixes, 1)
    run(query_piece, 0)
    run(stage_c, 3)
    run(stage_f, 2, 2)
    run(query_piece, 1)
    run(wait_prefixes, 0)
    run(retention, 1, 0)
    run(stage_d, 4, 0)
    run(retention, 0, 0)
    run(wait_prefixes, 1)
    run(stage_d, 3, 1)
    run(retention, 1, 1)
    run(stage_d, 3, 0)
    run(stage_d, 3, 2)
    run(retention, 0, 1)
    run(stage_e, 4, 0)
    run(stage_e, 3, 1)
    run(wait_retained)
    run(out_piece, c, 0)
    run(stage_f, 4, 0)
    run(stage_e, 3, 0)
    run(out_piece, other, 0)
    run(out_piece, c, 3)
    run(stage_e, 3, 2)
    run(stage_f, 3, 1)
    run(out_piece, other, 3)
    run(stage_f, 3, 2)
    run(out_piece, c, 2)
    run(stage_f, 3, 0)
    run(out_piece, c, 1)
    run(out_piece, other, 2)
    run(out_piece, other, 1)

    for wave in range(WAVES):
        finish_sends(wave)
    for half in range(2):
        drain(s_recv.at[half, pl.ds(0, SHARDS - 1)], ss.at[half])
        drain(p_recv.at[half, pl.ds(0, SHARDS - 1)], ps.at[half])
    for h in range(4):
        drain(ret_send.at[0], rs.at[h])
    for j in range(8):
        drain(w.at[0], os.at[j])


def body(tokens, norm_gain, w_query, w_key, w_value, w_out, decay_rate):
    high, low = rope_constants()
    any_spec = pl.BlockSpec(memory_space=pl.ANY)
    dma = pltpu.SemaphoreType.DMA
    scratch = [
        pltpu.VMEM((PIECES + 8, 4, 4, 4, 32, 128), BF16),
        pltpu.VMEM((PIECES, 16, 128), BF16),
        pltpu.VMEM((LEN, D), BF16),
        pltpu.VMEM((2, LEN, D), BF16),
        pltpu.VMEM((1, D), F32),
        pltpu.VMEM((2, 16, DK), F32),
        pltpu.VMEM((2, 32, DK), F32),
        pltpu.VMEM((HEADS, 64), F32),
        pltpu.VMEM((HEADS, 64), F32),
        pltpu.VMEM((LEN, DK), F32),
        pltpu.VMEM((LEN, DK), F32),
        pltpu.VMEM((2, 4, 4, 128), F32),
        pltpu.VMEM((2, 5, 4, 128), F32),
        pltpu.VMEM((2, 4, SHARDS, 128), F32),
        pltpu.VMEM((2, 4, LEN, DK), BF16),
        pltpu.VMEM((2, 4, LEN, DK), BF16),
        pltpu.VMEM((2, 4, LEN, DV), BF16),
        pltpu.VMEM((2, SHARDS, 32, DV), BF16),
        pltpu.VMEM((2, SHARDS, 32, DV), BF16),
        pltpu.VMEM((2, SHARDS, 32, DV), BF16),
        pltpu.VMEM((2, SHARDS, 32, DV), BF16),
        pltpu.VMEM((LEN, D), BF16),
        pltpu.VMEM((4, LEN, DV), BF16),
        dma((4,)), dma((4,)), dma((WAVES,)), dma((WAVES,)), dma((WAVES,)), dma, dma, dma((4,)), dma((4,)),
        dma((WAVES,)), dma((WAVES,)), dma((WAVES,)), dma((WAVES,)), dma((WAVES,)), dma((WAVES,)),
        dma((WAVES,)), dma((WAVES, 3, 2, 2)), dma((WAVES, 3)), dma((WAVES, 3, 2)),
        dma((2,)), dma((2,)), dma((2,)), dma((2,)), dma((4,)), dma((4,)), dma((8,)), dma((8,)),
    ]
    args = (
        tokens, norm_gain[None], w_query, w_key, w_value, w_out, decay_rate[0],
        jnp.asarray(high), jnp.asarray(low),
    )
    return pl.pallas_call(
        kernel,
        out_shape=jax.ShapeDtypeStruct((1, LEN, D), BF16),
        in_specs=[any_spec] * 9,
        out_specs=pl.BlockSpec(memory_space=pltpu.VMEM),
        scratch_shapes=scratch,
        compiler_params=pltpu.CompilerParams(
            collective_id=0, has_side_effects=True, vmem_limit_bytes=44 * 1024 * 1024
        ),
    )(*(pltpu.with_memory_space_constraint(a, pltpu.HBM) for a in args))


def solution(mesh):
    split = Mesh(mesh.devices.reshape(4, 4, 4, 2), ("z", "y", "x", "c"))
    in_specs = (
        P(("x", "c"), ("z", "y"), None),
        P(),
        P(("z", "y", "x", "c"), None),
        P(("z", "y", "x", "c"), None),
        P(("z", "y", "x", "c"), None),
        P(("z", "y", "x", "c"), None),
        P(("x", "c"), None, None),
    )
    return jax.shard_map(
        body, mesh=split, in_specs=in_specs, out_specs=P(("x", "c"), ("z", "y"), None), check_vma=False
    )
```

```python
import functools

import jax
import jax.numpy as jnp
import numpy as np
from jax import lax
from jax.experimental import pallas as pl
from jax.experimental.pallas import tpu as pltpu
from jax.sharding import Mesh
from jax.sharding import PartitionSpec as P

MESH = pl.DeviceIdType.MESH
F32 = jnp.float32
BF16 = jnp.bfloat16

HEADS = 8
DK = 128
DV = 256
BLOCK = 128
D = 2048
LEN = 512
SHARDS = 16
EPS_RMS = 1e-06
EPS_GROUP = 0.01
ROPE_BASE = 10000.0

PLAN = (
    (((1, 2, 0), "V"), ((0, 1, 2), "K"), ((2, 0, 1), "V")),
    (((2, 1, 0), "KV"), ((1, 0, 2), "KKV"), ((0, 2, 1), "VV")),
    (((2, 1, 0), "QQ"), ((0, 2, 1), "VV"), ((1, 0, 2), "QQOO")),
    (((2, 0, 1), "OO"), ((2, 1, 0), "O"), ((2, 1, 0), "O")),
    (((0, 1, 2), "OO"), ((2, 1, 0), ""), ((1, 0, 2), "")),
)
WAVES = len(PLAN)
PIECES = 24
KINDS = "".join(kinds for wave in PLAN for _, kinds in wave)


def ranges():
    at, parts, whole = 0, [], []
    for wave in PLAN:
        first, mine = at, []
        for order, kinds in wave:
            mine.append((order, at, len(kinds)))
            at += len(kinds)
        parts.append(mine)
        whole.append((first, at - first))
    return parts, whole


PARTS, WHOLE = ranges()
AT = {kind: [i for i, k in enumerate(KINDS) if k == kind] for kind in "KVQO"}


def rope_constants():
    inverse = ROPE_BASE ** (-(np.arange(DK // 2, dtype=np.float64) / (DK // 2 - 1)))
    inverse = np.repeat(inverse, 2)
    high = np.arange(256, dtype=np.float64)[:, None] * 32 * inverse[None, :]
    low = np.arange(32, dtype=np.float64)[:, None] * inverse[None, :]
    high = np.stack([np.cos(high), np.sin(high)]).astype(np.float32)
    low = np.stack([np.cos(low), np.sin(low)]).astype(np.float32)
    return high, low


def kernel(
    tokens, gain_in, wq, wk, wv, wo, rates_in, high_in, low_in,
    out,
    w, for_mate, x_raw, xn, gain, high, low, rates, rates2, cos_t, sin_t, rate_b, base_b, dec,
    keys, queries, values, s_send, s_recv, p_send, p_recv, ret, ret_send,
    in_sem, tok_sem, own_sem, mate_s, mate_r, rate_s, rate_r, xn_s, xn_r,
    p1s, p1r, p2s, p2r, p2fs, p2fr, p3s, p3r, p3fs, p3fr,
    ss, sr, ps, pr, rs, rr, os, orr,
):
    z, y, x, c = (lax.axis_index(a) for a in ("z", "y", "x", "c"))
    here = (z, y, x)
    shard = z * 4 + y
    mate = (z, y, x, 1 - c)

    def device(dim, step, core=None):
        at = list(here)
        at[dim] = lax.rem(at[dim] + step, 4)
        return (*at, c if core is None else core)

    def peer(step):
        to = lax.rem(shard + step, SHARDS)
        return to, (lax.div(to, 4), lax.rem(to, 4), x, c)

    tok_copies = []
    for i in range(4):
        rows = pl.ds(i * 128, 128)
        cp = pltpu.make_async_copy(tokens.at[0, rows], x_raw.at[rows], tok_sem.at[i])
        tok_copies.append(cp)

    def columns_of(piece, core):
        kind = KINDS[piece]
        i = AT[kind].index(piece)
        if kind == "V":
            ref, at = wv, core * 512 + (i % 2 * 1024 + i // 2 * 128)
        elif kind == "O":
            ref, at = wo, core * 1024 + i * 128
        else:
            ref, at = wk if kind == "K" else wq, core * 512 + i * 128
        return ref.at[:, pl.ds(pl.multiple_of(at, 128), 128)]

    own_rows = pl.ds(pl.multiple_of(c * 16, 16), 16)
    other = 1 - c

    barrier = pltpu.get_barrier_semaphore()
    first_peers = [mate]
    for dim in range(3):
        for step in (2, 1, 3):
            first_peers += [device(dim, step), device(dim, step, other)]
    for dev in first_peers:
        pl.semaphore_signal(barrier, inc=1, device_id=dev, device_id_type=MESH)

    in_copies = [
        pltpu.make_async_copy(gain_in, gain, in_sem.at[0]),
        pltpu.make_async_copy(rates_in, rates, in_sem.at[1]),
        pltpu.make_async_copy(high_in.at[:, pl.ds(pl.multiple_of(shard * 16, 16), 16)], high, in_sem.at[2]),
        pltpu.make_async_copy(low_in, low, in_sem.at[3]),
    ]
    for wave, (first, count) in enumerate(WHOLE):
        for piece in range(first, first + count):
            pltpu.make_async_copy(columns_of(piece, c), w.at[piece, z, y, x, own_rows], own_sem.at[wave]).start()
            pltpu.make_async_copy(columns_of(piece, other), for_mate.at[piece], own_sem.at[wave]).start()
        if wave == 0:
            for cp in in_copies:
                cp.start()
    for cp in tok_copies:
        cp.start()
    pl.semaphore_wait(barrier, len(first_peers))
    rate_copy = pltpu.make_async_remote_copy(
        rates_in, rates2, rate_s, rate_r, device_id=mate, device_id_type=MESH
    )

    def part_slice(first, count, where):
        return w.at[(pl.ds(first, count), *(where.get(d, pl.ds(0, 4)) for d in range(3)))]

    def send(src, ssem, rsem, dev):
        pltpu.make_async_remote_copy(src, src, ssem, rsem, device_id=dev, device_id_type=MESH).start()

    def drain(ref, sem):
        pltpu.make_async_copy(ref, ref, sem).wait()

    def rows_of(wave):
        return pl.ds(*WHOLE[wave])

    def p1_wait_ref(wave):
        return w.at[rows_of(wave), 0, 0, pl.ds(0, 3)]

    def p2_wait_ref(wave):
        return w.at[rows_of(wave), pl.ds(0, 2), 0]

    def p2f_wait_ref(wave):
        return w.at[rows_of(wave), 0, 0]

    def mate_wait_ref(wave):
        return w.at[rows_of(wave), 0, 0, 0, pl.ds(0, 16)]

    def half_wait_ref(count):
        return w.at[pl.ds(0, count), pl.ds(0, 2), 0]

    HALF = (pl.ds(0, 2), pl.ds(2, 2))

    def parts_of(wave):
        return [(part, *it) for part, it in enumerate(PARTS[wave]) if it[2]]

    def stage_p(wave):
        drain(w.at[rows_of(wave), 0, 0, 0], own_sem.at[wave])
        for part, (d1, d2, d3), first, count in parts_of(wave):
            pieces = pl.ds(first, count)
            own = w.at[pieces, z, y, x, own_rows]
            theirs = for_mate.at[pieces]
            pltpu.make_async_remote_copy(
                theirs, own, mate_s.at[wave], mate_r.at[wave, part], device_id=mate, device_id_type=MESH
            ).start()
            for step in (2, 1, 3):
                for src, core in ((own, c), (theirs, other)):
                    pltpu.make_async_remote_copy(
                        src, own, p1s.at[wave], p1r.at[wave, part],
                        device_id=device(d1, step, core), device_id_type=MESH,
                    ).start()

    def stage_a(wave):
        for part, (d1, d2, d3), first, count in parts_of(wave):
            pieces = pl.ds(first, count)
            drain(w.at[pieces, 0, 0, 0, pl.ds(0, 16)], mate_r.at[wave, part])
            drain(w.at[pieces, 0, 0, pl.ds(0, 3)], p1r.at[wave, part])
            own = part_slice(first, count, {d2: here[d2], d3: here[d3]})
            for step in (1, 3):
                send(own, p2s.at[wave], p2r.at[wave, part], device(d2, step))

    def stage_b(wave):
        for part, (d1, d2, d3), first, count in parts_of(wave):
            drain(w.at[pl.ds(first, count), pl.ds(0, 2), 0], p2r.at[wave, part])
            for i, step in enumerate((1, 3)):
                origin = lax.rem(here[d2] + 4 - step, 4)
                src = part_slice(first, count, {d1: HALF[i], d2: origin, d3: here[d3]})
                send(src, p2fs.at[wave], p2fr.at[wave, part], device(d2, step))

    def stage_c(wave):
        for sub in range(2):
            for part, (d1, d2, d3), first, count in parts_of(wave):
                if sub == 0:
                    drain(w.at[pl.ds(first, count), 0, 0], p2fr.at[wave, part])
                for i, step in enumerate((1, 3)):
                    half = sub if i == 0 else 1 - sub
                    src = part_slice(first, count, {d2: HALF[half], d3: here[d3]})
                    send(src, p3s.at[wave], p3r.at[wave, part, i, sub], device(d3, step))
        for part, (d1, d2, d3), first, count in parts_of(wave):
            pass_on(first, count, d3, here[d3])

    def stage_d(wave, part):
        (d1, d2, d3), first, count = PARTS[wave][part]
        for i, step in enumerate((1, 3)):
            drain(half_wait_ref(count), p3r.at[wave, part, i, 0])
            origin = lax.rem(here[d3] + 4 - step, 4)
            src = part_slice(first, count, {d2: HALF[i], d3: origin})
            send(src, p3fs.at[wave, part], p3fr.at[wave, part, i], device(d3, step))

    def pass_on(first, count, d3, at):
        for piece in range(first, first + count):
            if KINDS[piece] == "O":
                j = AT["O"].index(piece)
                pltpu.make_async_remote_copy(
                    part_slice(piece, 1, {d3: at}), part_slice(PIECES + j, 1, {d3: at}),
                    os.at[j], orr.at[j], device_id=mate, device_id_type=MESH,
                ).start()

    def stage_e(wave, part):
        (d1, d2, d3), first, count = PARTS[wave][part]
        for i, step in enumerate((1, 3)):
            drain(half_wait_ref(count), p3r.at[wave, part, i, 1])
            pass_on(first, count, d3, lax.rem(here[d3] + 4 - step, 4))

    def stage_f(wave, part):
        (d1, d2, d3), first, count = PARTS[wave][part]
        for i in range(2):
            drain(half_wait_ref(count), p3fr.at[wave, part, i])
        pass_on(first, count, d3, lax.rem(here[d3] + 2, 4))

    def finish_sends(wave):
        drain(mate_wait_ref(wave), mate_s.at[wave])
        drain(p1_wait_ref(wave), p1s.at[wave])
        drain(p2_wait_ref(wave), p2s.at[wave])
        drain(p2f_wait_ref(wave), p2fs.at[wave])
        drain(w.at[rows_of(wave), pl.ds(0, 2)], p3s.at[wave])
        for part, order, first, count in parts_of(wave):
            drain(w.at[pl.ds(first, count), 0], p3fs.at[wave, part])

    def norm(i):
        rows = pl.ds(i * 128, 128)
        tok_copies[i].wait()
        wide = x_raw[rows].astype(F32)
        inv = lax.rsqrt(jnp.sum(wide * wide, axis=-1, keepdims=True) * (1.0 / D) + EPS_RMS)
        xn[0, rows] = (wide * inv * gain[...]).astype(BF16)

    def norm_copy(i):
        rows = pl.ds(i * 128, 128)
        return pltpu.make_async_remote_copy(
            xn.at[0, rows], xn.at[1, rows], xn_s.at[i], xn_r.at[i], device_id=mate, device_id_type=MESH
        )

    def tables():
        lane = lax.broadcasted_iota(jnp.int32, (32, DK), 1)
        sign = jnp.where(lax.rem(lane, 2) == 0, -1.0, 1.0).astype(F32)
        cl, sl = low[0], low[1]
        for i in range(16):
            ch, sh = high[0, pl.ds(i, 1)], high[1, pl.ds(i, 1)]
            cos_t[pl.ds(i * 32, 32)] = ch * cl - sh * sl
            sin_t[pl.ds(i * 32, 32)] = (sh * cl + ch * sl) * sign

    def decays():
        lane = lax.broadcasted_iota(jnp.int32, (4, 64), 1)
        for s in range(2):
            full = rates[...] if s == 0 else rates2[...]
            mine = jnp.where(c == 0, full[0:4], full[4:8])
            base = jnp.zeros((4, 1), F32)
            for n in range(4):
                r = jnp.sum(jnp.where(lane == shard * 4 + n, mine, 0.0), axis=1, keepdims=True)
                rate_b[s, n] = jnp.broadcast_to(r, (4, 128))
                base_b[s, n] = jnp.broadcast_to(base, (4, 128))
                base = base + r * float(BLOCK)
            base_b[s, 4] = jnp.broadcast_to(base, (4, 128))
            for t in range(SHARDS - 1):
                tot = jnp.sum(jnp.where(lax.div(lane, 4) == t, mine, 0.0), axis=1, keepdims=True)
                e = jnp.broadcast_to(jnp.exp(tot * (-float(BLOCK))), (4, 128))
                for h in range(4):
                    dec[h // 2, s * 2 + h % 2, pl.ds(t, 1)] = e[h : h + 1]

    def turned(prod, s, h, sign, scale):
        v = prod.astype(BF16).astype(F32)
        even = lax.rem(lax.broadcasted_iota(jnp.int32, v.shape, 1), 2) == 0
        swap = jnp.where(even, pltpu.roll(v, DK - 1, 1), pltpu.roll(v, 1, 1))
        rot = v * cos_t[...] + swap * sin_t[...]
        offset = (lax.broadcasted_iota(jnp.int32, (BLOCK, DK), 0) + 1).astype(F32)
        parts = []
        for n in range(4):
            e = base_b[s, n, pl.ds(h, 1)] + rate_b[s, n, pl.ds(h, 1)] * offset
            parts.append(rot[n * BLOCK : (n + 1) * BLOCK] * (jnp.exp(e * sign) * scale))
        return jnp.concatenate(parts, axis=0).astype(BF16)

    def pair(pieces):
        return jnp.concatenate([w[piece].reshape(D, 128) for piece in pieces], axis=1)

    def project(kind, j):
        return jnp.dot(
            xn[...].reshape(2 * LEN, D), pair(AT[kind][2 * j : 2 * j + 2]), preferred_element_type=F32
        ).reshape(2, LEN, 256)

    def key_piece(j):
        prod = project("K", j)
        for s in range(2):
            for hh in range(2):
                h = 2 * j + hh
                keys[s, h] = turned(prod[s, :, hh * 128 : (hh + 1) * 128], s, h, 1.0, DK ** (-0.5))

    def query_piece(j):
        prod = project("Q", j)
        for s in range(2):
            for hh in range(2):
                h = 2 * j + hh
                queries[s, h] = turned(prod[s, :, hh * 128 : (hh + 1) * 128], s, h, -1.0, 1.0)

    def value_piece(h):
        prod = project("V", h)
        for s in range(2):
            values[s, h] = prod[s].astype(BF16)

    def local_states(half):
        for p in range(4):
            s, h = p // 2, half * 2 + p % 2
            st = lax.dot_general(
                keys[s, h], values[s, h], (((0,), (0,)), ((), ())), preferred_element_type=F32
            )
            e = jnp.exp(-base_b[s, 4, pl.ds(h, 1)])
            e = jnp.concatenate([e, e], axis=1)
            s_send[half, pl.ds(p * 4, 4)] = (st * e).astype(BF16).reshape(4, 32, DV)
        s_recv[half, shard] = s_send[half, shard]

    def send_states(half):
        def body(step, carry):
            to, dev = peer(step)
            pltpu.make_async_remote_copy(
                s_send.at[half, to], s_recv.at[half, shard], ss.at[half], sr.at[half],
                device_id=dev, device_id_type=MESH,
            ).start()
            return carry
        lax.fori_loop(1, SHARDS, body, 0)

    def scan_states(half):
        drain(s_recv.at[half, pl.ds(0, SHARDS - 1)], sr.at[half])
        run = jnp.zeros((32, DV), F32)
        rows = dec[half, z]
        for t in range(SHARDS):
            p_send[half, t] = run.astype(BF16)
            if t < SHARDS - 1:
                e = rows[t : t + 1]
                run = run * jnp.concatenate([e, e], axis=1) + s_recv[half, t].astype(F32)
        p_recv[half, shard] = p_send[half, shard]

    def send_prefixes(half):
        def body(step, carry):
            to, dev = peer(step)
            pltpu.make_async_remote_copy(
                p_send.at[half, to], p_recv.at[half, shard], ps.at[half], pr.at[half],
                device_id=dev, device_id_type=MESH,
            ).start()
            return carry
        lax.fori_loop(1, SHARDS, body, 0)

    def retention(s, half):
        row = lax.broadcasted_iota(jnp.int32, (256, 256), 0)
        col = lax.broadcasted_iota(jnp.int32, (256, 256), 1)
        for hh in range(2):
            h = half * 2 + hh
            p = s * 2 + hh
            before = p_recv[half, pl.ds(p * 4, 4)].reshape(DK, DV)
            for i in range(2):
                q = queries[s, h, pl.ds(i * 256, 256)]
                mixed = jnp.dot(q, before, preferred_element_type=F32)
                for j in range(i + 1):
                    k = keys[s, h, pl.ds(j * 256, 256)]
                    sc = lax.dot_general(q, k, (((1,), (1,)), ((), ())), preferred_element_type=F32)
                    if i == j:
                        sc = jnp.where(row >= col, sc, 0.0)
                    mixed = mixed + jnp.dot(
                        sc.astype(BF16), values[s, h, pl.ds(j * 256, 256)], preferred_element_type=F32
                    )
                mu = jnp.sum(mixed, axis=1, keepdims=True) * (1.0 / DV)
                sq = jnp.sum(mixed * mixed, axis=1, keepdims=True) * (1.0 / DV)
                done = ((mixed - mu) * lax.rsqrt(sq - mu * mu + EPS_GROUP)).astype(BF16)
                rows = pl.ds(i * 256, 256)
                if s == 0:
                    for g in range(2):
                        at = pl.multiple_of((g * HEADS + c * 4 + h) * 128, 128)
                        ret[rows, pl.ds(at, 128)] = done[:, g * 128 : (g + 1) * 128]
                else:
                    ret_send[h, rows] = done
            if s == 1:
                for g in range(2):
                    at = pl.multiple_of((g * HEADS + c * 4 + h) * 128, 128)
                    pltpu.make_async_remote_copy(
                        ret_send.at[h, :, pl.ds(g * 128, 128)], ret.at[:, pl.ds(at, 128)],
                        rs.at[h], rr.at[h], device_id=mate, device_id_type=MESH,
                    ).start()

    def out_piece(core, j):
        pieces = (2 * j, 2 * j + 1)
        if core is c:
            pieces = [AT["O"][i] for i in pieces]
        else:
            for i in pieces:
                drain(w.at[0], orr.at[i])
            pieces = [PIECES + i for i in pieces]
        prod = jnp.dot(ret[...], pair(pieces), preferred_element_type=F32)
        at = pl.multiple_of(core * 1024 + j * 256, 256)
        out[0, :, pl.ds(at, 256)] = prod.astype(BF16)

    def wait_prefixes(half):
        drain(p_recv.at[half, pl.ds(0, SHARDS - 1)], pr.at[half])

    def wait_retained():
        for h in range(4):
            drain(ret_send.at[0], rr.at[h])

    def wait_inputs():
        for cp in in_copies:
            cp.wait()

    def send_rates():
        rate_copy.start()

    def wait_rates():
        rate_copy.wait()

    def send_normed(i):
        norm_copy(i).start()

    def wait_normed():
        for i in range(4):
            norm_copy(i).wait()

    compute = (
        norm, tables, decays, key_piece, query_piece, value_piece,
        local_states, scan_states, retention, out_piece,
    )

    def run(step, *args):
        with jax.named_scope(step.__name__ + "".join(f"_{a}" for a in args if isinstance(a, int))):
            if step in compute:
                pl.when(z < 4)(functools.partial(step, *args))
            else:
                step(*args)

    run(stage_p, 0)
    run(stage_p, 1)
    run(stage_p, 2)
    run(stage_p, 3)
    run(stage_p, 4)
    run(stage_a, 0)
    run(stage_a, 1)
    run(stage_b, 0)
    run(send_rates)
    run(stage_a, 4)
    run(wait_inputs)
    run(norm, 0)
    run(stage_a, 2)
    run(norm, 1)
    run(stage_b, 1)
    run(norm, 2)
    run(send_normed, 2)
    run(stage_c, 0)
    run(stage_b, 2)
    run(send_normed, 1)
    run(tables)
    run(stage_c, 1)
    run(send_normed, 0)
    run(stage_d, 0, 2)
    run(norm, 3)
    run(stage_d, 1, 2)
    run(stage_d, 0, 1)
    run(stage_e, 0, 2)
    run(stage_d, 0, 0)
    run(wait_rates)
    run(decays)
    run(stage_d, 1, 0)
    run(send_normed, 3)
    run(wait_normed)
    run(stage_e, 0, 0)
    run(stage_e, 1, 0)
    run(stage_d, 1, 1)
    run(stage_e, 1, 2)
    run(stage_c, 2)
    run(stage_f, 1, 0)
    run(stage_f, 0, 0)
    run(stage_e, 0, 1)
    run(stage_f, 0, 1)
    run(key_piece, 0)
    run(stage_f, 0, 2)
    run(stage_d, 2, 1)
    run(value_piece, 0)
    run(stage_d, 2, 0)
    run(stage_b, 4)
    run(stage_e, 1, 1)
    run(stage_f, 1, 2)
    run(value_piece, 2)
    run(stage_a, 3)
    run(stage_f, 1, 1)
    run(value_piece, 1)
    run(local_states, 0)
    run(send_states, 0)
    run(key_piece, 1)
    run(stage_e, 2, 1)
    run(stage_e, 2, 0)
    run(stage_f, 2, 1)
    run(value_piece, 3)
    run(stage_d, 2, 2)
    run(local_states, 1)
    run(stage_f, 2, 0)
    run(send_states, 1)
    run(stage_b, 3)
    run(scan_states, 0)
    run(send_prefixes, 0)
    run(scan_states, 1)
    run(send_prefixes, 1)
    run(stage_c, 4)
    run(query_piece, 0)
    run(stage_e, 2, 2)
    run(stage_c, 3)
    run(stage_f, 2, 2)
    run(query_piece, 1)
    run(wait_prefixes, 0)
    run(retention, 1, 0)
    run(wait_prefixes, 1)
    run(stage_d, 4, 0)
    run(retention, 1, 1)
    run(stage_d, 3, 0)
    run(stage_d, 3, 2)
    run(retention, 0, 1)
    run(stage_e, 4, 0)
    run(stage_d, 3, 1)
    run(retention, 0, 0)
    run(stage_e, 3, 1)
    run(wait_retained)
    run(out_piece, c, 0)
    run(stage_f, 4, 0)
    run(stage_e, 3, 0)
    run(out_piece, other, 0)
    run(out_piece, c, 3)
    run(stage_e, 3, 2)
    run(stage_f, 3, 2)
    run(out_piece, other, 3)
    run(stage_f, 3, 1)
    run(stage_f, 3, 0)
    run(out_piece, c, 2)
    run(out_piece, c, 1)
    run(out_piece, other, 2)
    run(out_piece, other, 1)

    for wave in range(WAVES):
        finish_sends(wave)
    for half in range(2):
        drain(s_recv.at[half, pl.ds(0, SHARDS - 1)], ss.at[half])
        drain(p_recv.at[half, pl.ds(0, SHARDS - 1)], ps.at[half])
    for h in range(4):
        drain(ret_send.at[0], rs.at[h])
    for j in range(8):
        drain(w.at[0], os.at[j])


def body(tokens, norm_gain, w_query, w_key, w_value, w_out, decay_rate):
    high, low = rope_constants()
    any_spec = pl.BlockSpec(memory_space=pl.ANY)
    dma = pltpu.SemaphoreType.DMA
    scratch = [
        pltpu.VMEM((PIECES + 8, 4, 4, 4, 32, 128), BF16),
        pltpu.VMEM((PIECES, 16, 128), BF16),
        pltpu.VMEM((LEN, D), BF16),
        pltpu.VMEM((2, LEN, D), BF16),
        pltpu.VMEM((1, D), F32),
        pltpu.VMEM((2, 16, DK), F32),
        pltpu.VMEM((2, 32, DK), F32),
        pltpu.VMEM((HEADS, 64), F32),
        pltpu.VMEM((HEADS, 64), F32),
        pltpu.VMEM((LEN, DK), F32),
        pltpu.VMEM((LEN, DK), F32),
        pltpu.VMEM((2, 4, 4, 128), F32),
        pltpu.VMEM((2, 5, 4, 128), F32),
        pltpu.VMEM((2, 4, SHARDS, 128), F32),
        pltpu.VMEM((2, 4, LEN, DK), BF16),
        pltpu.VMEM((2, 4, LEN, DK), BF16),
        pltpu.VMEM((2, 4, LEN, DV), BF16),
        pltpu.VMEM((2, SHARDS, 32, DV), BF16),
        pltpu.VMEM((2, SHARDS, 32, DV), BF16),
        pltpu.VMEM((2, SHARDS, 32, DV), BF16),
        pltpu.VMEM((2, SHARDS, 32, DV), BF16),
        pltpu.VMEM((LEN, D), BF16),
        pltpu.VMEM((4, LEN, DV), BF16),
        dma((4,)), dma((4,)), dma((WAVES,)), dma((WAVES,)), dma((WAVES, 3)), dma, dma, dma((4,)), dma((4,)),
        dma((WAVES,)), dma((WAVES, 3)), dma((WAVES,)), dma((WAVES, 3)), dma((WAVES,)), dma((WAVES, 3)),
        dma((WAVES,)), dma((WAVES, 3, 2, 2)), dma((WAVES, 3)), dma((WAVES, 3, 2)),
        dma((2,)), dma((2,)), dma((2,)), dma((2,)), dma((4,)), dma((4,)), dma((8,)), dma((8,)),
    ]
    args = (
        tokens, norm_gain[None], w_query, w_key, w_value, w_out, decay_rate[0],
        jnp.asarray(high), jnp.asarray(low),
    )
    return pl.pallas_call(
        kernel,
        out_shape=jax.ShapeDtypeStruct((1, LEN, D), BF16),
        in_specs=[any_spec] * 9,
        out_specs=pl.BlockSpec(memory_space=pltpu.VMEM),
        scratch_shapes=scratch,
        compiler_params=pltpu.CompilerParams(
            collective_id=0, has_side_effects=True, vmem_limit_bytes=44 * 1024 * 1024
        ),
    )(*(pltpu.with_memory_space_constraint(a, pltpu.HBM) for a in args))


def solution(mesh):
    split = Mesh(mesh.devices.reshape(4, 4, 4, 2), ("z", "y", "x", "c"))
    in_specs = (
        P(("x", "c"), ("z", "y"), None),
        P(),
        P(("z", "y", "x", "c"), None),
        P(("z", "y", "x", "c"), None),
        P(("z", "y", "x", "c"), None),
        P(("z", "y", "x", "c"), None),
        P(("x", "c"), None, None),
    )
    return jax.shard_map(
        body, mesh=split, in_specs=in_specs, out_specs=P(("x", "c"), ("z", "y"), None), check_vma=False
    )
```

```python
import functools

import jax
import jax.numpy as jnp
import numpy as np
from jax import lax
from jax.experimental import pallas as pl
from jax.experimental.pallas import tpu as pltpu
from jax.sharding import Mesh
from jax.sharding import PartitionSpec as P

MESH = pl.DeviceIdType.MESH
F32 = jnp.float32
BF16 = jnp.bfloat16

HEADS = 8
DK = 128
DV = 256
BLOCK = 128
D = 2048
LEN = 512
SHARDS = 16
EPS_RMS = 1e-06
EPS_GROUP = 0.01
ROPE_BASE = 10000.0

PLAN = (
    (((1, 2, 0), "V"), ((0, 1, 2), "K"), ((2, 0, 1), "V")),
    (((2, 1, 0), "KV"), ((1, 0, 2), "KKV"), ((0, 2, 1), "VV")),
    (((2, 1, 0), "QQ"), ((0, 2, 1), "VV"), ((1, 0, 2), "QQOO")),
    (((2, 0, 1), "OO"), ((2, 1, 0), "O"), ((2, 1, 0), "O")),
    (((0, 1, 2), "OO"), ((2, 1, 0), ""), ((1, 0, 2), "")),
)
WAVES = len(PLAN)
PIECES = 24
KINDS = "".join(kinds for wave in PLAN for _, kinds in wave)


def ranges():
    at, parts, whole = 0, [], []
    for wave in PLAN:
        first, mine = at, []
        for order, kinds in wave:
            mine.append((order, at, len(kinds)))
            at += len(kinds)
        parts.append(mine)
        whole.append((first, at - first))
    return parts, whole


PARTS, WHOLE = ranges()
AT = {kind: [i for i, k in enumerate(KINDS) if k == kind] for kind in "KVQO"}


def rope_constants():
    inverse = ROPE_BASE ** (-(np.arange(DK // 2, dtype=np.float64) / (DK // 2 - 1)))
    inverse = np.repeat(inverse, 2)
    high = np.arange(256, dtype=np.float64)[:, None] * 32 * inverse[None, :]
    low = np.arange(32, dtype=np.float64)[:, None] * inverse[None, :]
    high = np.stack([np.cos(high), np.sin(high)]).astype(np.float32)
    low = np.stack([np.cos(low), np.sin(low)]).astype(np.float32)
    return high, low


def kernel(
    tokens, gain_in, wq, wk, wv, wo, rates_in, high_in, low_in,
    out,
    w, for_mate, x_raw, xn, gain, high, low, rates, rates2, cos_t, sin_t, rate_b, base_b, dec,
    keys, queries, values, s_send, s_recv, p_send, p_recv, ret, ret_send,
    in_sem, tok_sem, own_sem, mate_s, mate_r, rate_s, rate_r, xn_s, xn_r,
    p1s, p1r, p2s, p2r, p2fs, p2fr, p3s, p3r, p3fs, p3fr,
    ss, sr, ps, pr, rs, rr, os, orr,
):
    z, y, x, c = (lax.axis_index(a) for a in ("z", "y", "x", "c"))
    here = (z, y, x)
    shard = z * 4 + y
    mate = (z, y, x, 1 - c)

    def device(dim, step, core=None):
        at = list(here)
        at[dim] = lax.rem(at[dim] + step, 4)
        return (*at, c if core is None else core)

    def peer(step):
        to = lax.rem(shard + step, SHARDS)
        return to, (lax.div(to, 4), lax.rem(to, 4), x, c)

    tok_copies = []
    for i in range(4):
        rows = pl.ds(i * 128, 128)
        cp = pltpu.make_async_copy(tokens.at[0, rows], x_raw.at[rows], tok_sem.at[i])
        tok_copies.append(cp)

    def columns_of(piece, core):
        kind = KINDS[piece]
        i = AT[kind].index(piece)
        if kind == "V":
            ref, at = wv, core * 512 + (i % 2 * 1024 + i // 2 * 128)
        elif kind == "O":
            ref, at = wo, core * 1024 + i * 128
        else:
            ref, at = wk if kind == "K" else wq, core * 512 + i * 128
        return ref.at[:, pl.ds(pl.multiple_of(at, 128), 128)]

    own_rows = pl.ds(pl.multiple_of(c * 16, 16), 16)
    other = 1 - c

    barrier = pltpu.get_barrier_semaphore()
    first_peers = [mate]
    for dim in range(3):
        for step in (2, 1, 3):
            first_peers += [device(dim, step), device(dim, step, other)]
    for dev in first_peers:
        pl.semaphore_signal(barrier, inc=1, device_id=dev, device_id_type=MESH)

    in_copies = [
        pltpu.make_async_copy(gain_in, gain, in_sem.at[0]),
        pltpu.make_async_copy(rates_in, rates, in_sem.at[1]),
        pltpu.make_async_copy(high_in.at[:, pl.ds(pl.multiple_of(shard * 16, 16), 16)], high, in_sem.at[2]),
        pltpu.make_async_copy(low_in, low, in_sem.at[3]),
    ]
    for wave, (first, count) in enumerate(WHOLE):
        for piece in range(first, first + count):
            pltpu.make_async_copy(columns_of(piece, c), w.at[piece, z, y, x, own_rows], own_sem.at[wave]).start()
            pltpu.make_async_copy(columns_of(piece, other), for_mate.at[piece], own_sem.at[wave]).start()
        if wave == 0:
            for cp in in_copies:
                cp.start()
    for cp in tok_copies:
        cp.start()
    pl.semaphore_wait(barrier, len(first_peers))
    rate_copy = pltpu.make_async_remote_copy(
        rates_in, rates2, rate_s, rate_r, device_id=mate, device_id_type=MESH
    )

    def part_slice(first, count, where):
        return w.at[(pl.ds(first, count), *(where.get(d, pl.ds(0, 4)) for d in range(3)))]

    def send(src, ssem, rsem, dev):
        pltpu.make_async_remote_copy(src, src, ssem, rsem, device_id=dev, device_id_type=MESH).start()

    def drain(ref, sem):
        pltpu.make_async_copy(ref, ref, sem).wait()

    def rows_of(wave):
        return pl.ds(*WHOLE[wave])

    def p1_wait_ref(wave):
        return w.at[rows_of(wave), 0, 0, pl.ds(0, 3)]

    def p2_wait_ref(wave):
        return w.at[rows_of(wave), pl.ds(0, 2), 0]

    def p2f_wait_ref(wave):
        return w.at[rows_of(wave), 0, 0]

    def mate_wait_ref(wave):
        return w.at[rows_of(wave), 0, 0, 0, pl.ds(0, 16)]

    def half_wait_ref(count):
        return w.at[pl.ds(0, count), pl.ds(0, 2), 0]

    HALF = (pl.ds(0, 2), pl.ds(2, 2))

    def parts_of(wave):
        return [(part, *it) for part, it in enumerate(PARTS[wave]) if it[2]]

    def stage_p(wave):
        drain(w.at[rows_of(wave), 0, 0, 0], own_sem.at[wave])
        for part, (d1, d2, d3), first, count in parts_of(wave):
            pieces = pl.ds(first, count)
            own = w.at[pieces, z, y, x, own_rows]
            theirs = for_mate.at[pieces]
            pltpu.make_async_remote_copy(
                theirs, own, mate_s.at[wave], mate_r.at[wave, part], device_id=mate, device_id_type=MESH
            ).start()
            for step in (2, 1, 3):
                for src, core in ((own, c), (theirs, other)):
                    pltpu.make_async_remote_copy(
                        src, own, p1s.at[wave], p1r.at[wave, part],
                        device_id=device(d1, step, core), device_id_type=MESH,
                    ).start()

    def stage_a(wave):
        for part, (d1, d2, d3), first, count in parts_of(wave):
            pieces = pl.ds(first, count)
            drain(w.at[pieces, 0, 0, 0, pl.ds(0, 16)], mate_r.at[wave, part])
            drain(w.at[pieces, 0, 0, pl.ds(0, 3)], p1r.at[wave, part])
            own = part_slice(first, count, {d2: here[d2], d3: here[d3]})
            for step in (1, 3):
                send(own, p2s.at[wave], p2r.at[wave, part], device(d2, step))

    def stage_b(wave):
        for part, (d1, d2, d3), first, count in parts_of(wave):
            drain(w.at[pl.ds(first, count), pl.ds(0, 2), 0], p2r.at[wave, part])
            for i, step in enumerate((1, 3)):
                origin = lax.rem(here[d2] + 4 - step, 4)
                src = part_slice(first, count, {d1: HALF[i], d2: origin, d3: here[d3]})
                send(src, p2fs.at[wave], p2fr.at[wave, part], device(d2, step))

    def stage_c(wave):
        for sub in range(2):
            for part, (d1, d2, d3), first, count in parts_of(wave):
                if sub == 0:
                    drain(w.at[pl.ds(first, count), 0, 0], p2fr.at[wave, part])
                for i, step in enumerate((1, 3)):
                    half = sub if i == 0 else 1 - sub
                    src = part_slice(first, count, {d2: HALF[half], d3: here[d3]})
                    send(src, p3s.at[wave], p3r.at[wave, part, i, sub], device(d3, step))
        for part, (d1, d2, d3), first, count in parts_of(wave):
            pass_on(first, count, d3, here[d3])

    def stage_d(wave, part):
        (d1, d2, d3), first, count = PARTS[wave][part]
        for i, step in enumerate((1, 3)):
            drain(half_wait_ref(count), p3r.at[wave, part, i, 0])
            origin = lax.rem(here[d3] + 4 - step, 4)
            src = part_slice(first, count, {d2: HALF[i], d3: origin})
            send(src, p3fs.at[wave, part], p3fr.at[wave, part, i], device(d3, step))

    def pass_on(first, count, d3, at):
        for piece in range(first, first + count):
            if KINDS[piece] == "O":
                j = AT["O"].index(piece)
                pltpu.make_async_remote_copy(
                    part_slice(piece, 1, {d3: at}), part_slice(PIECES + j, 1, {d3: at}),
                    os.at[j], orr.at[j], device_id=mate, device_id_type=MESH,
                ).start()

    def stage_e(wave, part):
        (d1, d2, d3), first, count = PARTS[wave][part]
        for i, step in enumerate((1, 3)):
            drain(half_wait_ref(count), p3r.at[wave, part, i, 1])
            pass_on(first, count, d3, lax.rem(here[d3] + 4 - step, 4))

    def stage_f(wave, part):
        (d1, d2, d3), first, count = PARTS[wave][part]
        for i in range(2):
            drain(half_wait_ref(count), p3fr.at[wave, part, i])
        pass_on(first, count, d3, lax.rem(here[d3] + 2, 4))

    def finish_sends(wave):
        drain(mate_wait_ref(wave), mate_s.at[wave])
        drain(p1_wait_ref(wave), p1s.at[wave])
        drain(p2_wait_ref(wave), p2s.at[wave])
        drain(p2f_wait_ref(wave), p2fs.at[wave])
        drain(w.at[rows_of(wave), pl.ds(0, 2)], p3s.at[wave])
        for part, order, first, count in parts_of(wave):
            drain(w.at[pl.ds(first, count), 0], p3fs.at[wave, part])

    def norm(i):
        rows = pl.ds(i * 128, 128)
        tok_copies[i].wait()
        wide = x_raw[rows].astype(F32)
        inv = lax.rsqrt(jnp.sum(wide * wide, axis=-1, keepdims=True) * (1.0 / D) + EPS_RMS)
        xn[0, rows] = (wide * inv * gain[...]).astype(BF16)

    def norm_copy(i):
        rows = pl.ds(i * 128, 128)
        return pltpu.make_async_remote_copy(
            xn.at[0, rows], xn.at[1, rows], xn_s.at[i], xn_r.at[i], device_id=mate, device_id_type=MESH
        )

    def tables():
        lane = lax.broadcasted_iota(jnp.int32, (32, DK), 1)
        sign = jnp.where(lax.rem(lane, 2) == 0, -1.0, 1.0).astype(F32)
        cl, sl = low[0], low[1]
        for i in range(16):
            ch, sh = high[0, pl.ds(i, 1)], high[1, pl.ds(i, 1)]
            cos_t[pl.ds(i * 32, 32)] = ch * cl - sh * sl
            sin_t[pl.ds(i * 32, 32)] = (sh * cl + ch * sl) * sign

    def decays():
        lane = lax.broadcasted_iota(jnp.int32, (4, 64), 1)
        for s in range(2):
            full = rates[...] if s == 0 else rates2[...]
            mine = jnp.where(c == 0, full[0:4], full[4:8])
            base = jnp.zeros((4, 1), F32)
            for n in range(4):
                r = jnp.sum(jnp.where(lane == shard * 4 + n, mine, 0.0), axis=1, keepdims=True)
                rate_b[s, n] = jnp.broadcast_to(r, (4, 128))
                base_b[s, n] = jnp.broadcast_to(base, (4, 128))
                base = base + r * float(BLOCK)
            base_b[s, 4] = jnp.broadcast_to(base, (4, 128))
            for t in range(SHARDS - 1):
                tot = jnp.sum(jnp.where(lax.div(lane, 4) == t, mine, 0.0), axis=1, keepdims=True)
                e = jnp.broadcast_to(jnp.exp(tot * (-float(BLOCK))), (4, 128))
                for h in range(4):
                    dec[h // 2, s * 2 + h % 2, pl.ds(t, 1)] = e[h : h + 1]

    def turned(prod, s, h, sign, scale):
        v = prod.astype(BF16).astype(F32)
        even = lax.rem(lax.broadcasted_iota(jnp.int32, v.shape, 1), 2) == 0
        swap = jnp.where(even, pltpu.roll(v, DK - 1, 1), pltpu.roll(v, 1, 1))
        rot = v * cos_t[...] + swap * sin_t[...]
        offset = (lax.broadcasted_iota(jnp.int32, (BLOCK, DK), 0) + 1).astype(F32)
        parts = []
        for n in range(4):
            e = base_b[s, n, pl.ds(h, 1)] + rate_b[s, n, pl.ds(h, 1)] * offset
            parts.append(rot[n * BLOCK : (n + 1) * BLOCK] * (jnp.exp(e * sign) * scale))
        return jnp.concatenate(parts, axis=0).astype(BF16)

    def pair(pieces):
        return jnp.concatenate([w[piece].reshape(D, 128) for piece in pieces], axis=1)

    def project(kind, j):
        return jnp.dot(
            xn[...].reshape(2 * LEN, D), pair(AT[kind][2 * j : 2 * j + 2]), preferred_element_type=F32
        ).reshape(2, LEN, 256)

    def key_piece(j):
        prod = project("K", j)
        for s in range(2):
            for hh in range(2):
                h = 2 * j + hh
                keys[s, h] = turned(prod[s, :, hh * 128 : (hh + 1) * 128], s, h, 1.0, DK ** (-0.5))

    def query_piece(j):
        prod = project("Q", j)
        for s in range(2):
            for hh in range(2):
                h = 2 * j + hh
                queries[s, h] = turned(prod[s, :, hh * 128 : (hh + 1) * 128], s, h, -1.0, 1.0)

    def value_piece(h):
        prod = project("V", h)
        for s in range(2):
            values[s, h] = prod[s].astype(BF16)

    def local_states(half):
        for p in range(4):
            s, h = p // 2, half * 2 + p % 2
            st = lax.dot_general(
                keys[s, h], values[s, h], (((0,), (0,)), ((), ())), preferred_element_type=F32
            )
            e = jnp.exp(-base_b[s, 4, pl.ds(h, 1)])
            e = jnp.concatenate([e, e], axis=1)
            s_send[half, pl.ds(p * 4, 4)] = (st * e).astype(BF16).reshape(4, 32, DV)
        s_recv[half, shard] = s_send[half, shard]

    def send_states(half):
        def body(step, carry):
            to, dev = peer(step)
            pltpu.make_async_remote_copy(
                s_send.at[half, to], s_recv.at[half, shard], ss.at[half], sr.at[half],
                device_id=dev, device_id_type=MESH,
            ).start()
            return carry
        lax.fori_loop(1, SHARDS, body, 0)

    def scan_states(half):
        drain(s_recv.at[half, pl.ds(0, SHARDS - 1)], sr.at[half])
        run = jnp.zeros((32, DV), F32)
        rows = dec[half, z]
        for t in range(SHARDS):
            p_send[half, t] = run.astype(BF16)
            if t < SHARDS - 1:
                e = rows[t : t + 1]
                run = run * jnp.concatenate([e, e], axis=1) + s_recv[half, t].astype(F32)
        p_recv[half, shard] = p_send[half, shard]

    def send_prefixes(half):
        def body(step, carry):
            to, dev = peer(step)
            pltpu.make_async_remote_copy(
                p_send.at[half, to], p_recv.at[half, shard], ps.at[half], pr.at[half],
                device_id=dev, device_id_type=MESH,
            ).start()
            return carry
        lax.fori_loop(1, SHARDS, body, 0)

    def retention(s, half):
        row = lax.broadcasted_iota(jnp.int32, (256, 256), 0)
        col = lax.broadcasted_iota(jnp.int32, (256, 256), 1)
        for hh in range(2):
            h = half * 2 + hh
            p = s * 2 + hh
            before = p_recv[half, pl.ds(p * 4, 4)].reshape(DK, DV)
            for i in range(2):
                q = queries[s, h, pl.ds(i * 256, 256)]
                mixed = jnp.dot(q, before, preferred_element_type=F32)
                for j in range(i + 1):
                    k = keys[s, h, pl.ds(j * 256, 256)]
                    sc = lax.dot_general(q, k, (((1,), (1,)), ((), ())), preferred_element_type=F32)
                    if i == j:
                        sc = jnp.where(row >= col, sc, 0.0)
                    mixed = mixed + jnp.dot(
                        sc.astype(BF16), values[s, h, pl.ds(j * 256, 256)], preferred_element_type=F32
                    )
                mu = jnp.sum(mixed, axis=1, keepdims=True) * (1.0 / DV)
                sq = jnp.sum(mixed * mixed, axis=1, keepdims=True) * (1.0 / DV)
                done = ((mixed - mu) * lax.rsqrt(sq - mu * mu + EPS_GROUP)).astype(BF16)
                rows = pl.ds(i * 256, 256)
                if s == 0:
                    for g in range(2):
                        at = pl.multiple_of((g * HEADS + c * 4 + h) * 128, 128)
                        ret[rows, pl.ds(at, 128)] = done[:, g * 128 : (g + 1) * 128]
                else:
                    ret_send[h, rows] = done
            if s == 1:
                for g in range(2):
                    at = pl.multiple_of((g * HEADS + c * 4 + h) * 128, 128)
                    pltpu.make_async_remote_copy(
                        ret_send.at[h, :, pl.ds(g * 128, 128)], ret.at[:, pl.ds(at, 128)],
                        rs.at[h], rr.at[h], device_id=mate, device_id_type=MESH,
                    ).start()

    def out_piece(core, j, count=1):
        pieces = range(2 * j, 2 * (j + count))
        if core is c:
            pieces = [AT["O"][i] for i in pieces]
        else:
            for i in pieces:
                drain(w.at[0], orr.at[i])
            pieces = [PIECES + i for i in pieces]
        prod = jnp.dot(ret[...], pair(pieces), preferred_element_type=F32)
        at = pl.multiple_of(core * 1024 + j * 256, 256)
        out[0, :, pl.ds(at, 256 * count)] = prod.astype(BF16)

    def wait_prefixes(half):
        drain(p_recv.at[half, pl.ds(0, SHARDS - 1)], pr.at[half])

    def wait_retained():
        for h in range(4):
            drain(ret_send.at[0], rr.at[h])

    def wait_inputs():
        for cp in in_copies:
            cp.wait()

    def send_rates():
        rate_copy.start()

    def wait_rates():
        rate_copy.wait()

    def send_normed(i):
        norm_copy(i).start()

    def wait_normed():
        for i in range(4):
            norm_copy(i).wait()

    compute = (
        norm, tables, decays, key_piece, query_piece, value_piece,
        local_states, scan_states, retention, out_piece,
    )

    def run(step, *args):
        with jax.named_scope(step.__name__ + "".join(f"_{a}" for a in args if isinstance(a, int))):
            if step in compute:
                pl.when(z < 4)(functools.partial(step, *args))
            else:
                step(*args)

    run(stage_p, 0)
    run(stage_p, 1)
    run(stage_p, 2)
    run(stage_p, 3)
    run(stage_p, 4)
    run(stage_a, 0)
    run(stage_a, 1)
    run(stage_b, 0)
    run(send_rates)
    run(stage_a, 4)
    run(wait_inputs)
    run(norm, 0)
    run(stage_a, 2)
    run(norm, 1)
    run(stage_b, 1)
    run(norm, 2)
    run(send_normed, 2)
    run(stage_c, 0)
    run(stage_b, 2)
    run(send_normed, 1)
    run(tables)
    run(stage_c, 1)
    run(send_normed, 0)
    run(stage_d, 0, 2)
    run(norm, 3)
    run(stage_d, 1, 2)
    run(stage_d, 0, 1)
    run(stage_e, 0, 2)
    run(stage_d, 0, 0)
    run(wait_rates)
    run(decays)
    run(stage_d, 1, 0)
    run(send_normed, 3)
    run(wait_normed)
    run(stage_e, 0, 0)
    run(stage_e, 1, 0)
    run(stage_d, 1, 1)
    run(stage_e, 1, 2)
    run(stage_c, 2)
    run(stage_f, 1, 0)
    run(stage_f, 0, 0)
    run(stage_e, 0, 1)
    run(stage_f, 0, 1)
    run(key_piece, 0)
    run(stage_f, 0, 2)
    run(stage_d, 2, 1)
    run(value_piece, 0)
    run(stage_d, 2, 0)
    run(stage_b, 4)
    run(stage_e, 1, 1)
    run(stage_f, 1, 2)
    run(value_piece, 2)
    run(stage_a, 3)
    run(stage_f, 1, 1)
    run(value_piece, 1)
    run(local_states, 0)
    run(send_states, 0)
    run(key_piece, 1)
    run(stage_e, 2, 1)
    run(stage_e, 2, 0)
    run(stage_f, 2, 1)
    run(value_piece, 3)
    run(stage_d, 2, 2)
    run(local_states, 1)
    run(stage_f, 2, 0)
    run(send_states, 1)
    run(stage_b, 3)
    run(scan_states, 0)
    run(send_prefixes, 0)
    run(scan_states, 1)
    run(send_prefixes, 1)
    run(stage_c, 4)
    run(query_piece, 0)
    run(stage_e, 2, 2)
    run(stage_c, 3)
    run(stage_f, 2, 2)
    run(query_piece, 1)
    run(wait_prefixes, 0)
    run(retention, 1, 0)
    run(wait_prefixes, 1)
    run(stage_d, 4, 0)
    run(retention, 1, 1)
    run(stage_d, 3, 0)
    run(stage_d, 3, 2)
    run(retention, 0, 1)
    run(stage_e, 4, 0)
    run(stage_d, 3, 1)
    run(retention, 0, 0)
    run(stage_e, 3, 1)
    run(wait_retained)
    run(out_piece, c, 0)
    run(stage_f, 4, 0)
    run(stage_e, 3, 0)
    run(out_piece, other, 0)
    run(out_piece, c, 3)
    run(stage_e, 3, 2)
    run(stage_f, 3, 2)
    run(out_piece, other, 3)
    run(stage_f, 3, 1)
    run(stage_f, 3, 0)
    run(out_piece, c, 1, 2)
    run(out_piece, other, 1, 2)

    for wave in range(WAVES):
        finish_sends(wave)
    for half in range(2):
        drain(s_recv.at[half, pl.ds(0, SHARDS - 1)], ss.at[half])
        drain(p_recv.at[half, pl.ds(0, SHARDS - 1)], ps.at[half])
    for h in range(4):
        drain(ret_send.at[0], rs.at[h])
    for j in range(8):
        drain(w.at[0], os.at[j])


def body(tokens, norm_gain, w_query, w_key, w_value, w_out, decay_rate):
    high, low = rope_constants()
    any_spec = pl.BlockSpec(memory_space=pl.ANY)
    dma = pltpu.SemaphoreType.DMA
    scratch = [
        pltpu.VMEM((PIECES + 8, 4, 4, 4, 32, 128), BF16),
        pltpu.VMEM((PIECES, 16, 128), BF16),
        pltpu.VMEM((LEN, D), BF16),
        pltpu.VMEM((2, LEN, D), BF16),
        pltpu.VMEM((1, D), F32),
        pltpu.VMEM((2, 16, DK), F32),
        pltpu.VMEM((2, 32, DK), F32),
        pltpu.VMEM((HEADS, 64), F32),
        pltpu.VMEM((HEADS, 64), F32),
        pltpu.VMEM((LEN, DK), F32),
        pltpu.VMEM((LEN, DK), F32),
        pltpu.VMEM((2, 4, 4, 128), F32),
        pltpu.VMEM((2, 5, 4, 128), F32),
        pltpu.VMEM((2, 4, SHARDS, 128), F32),
        pltpu.VMEM((2, 4, LEN, DK), BF16),
        pltpu.VMEM((2, 4, LEN, DK), BF16),
        pltpu.VMEM((2, 4, LEN, DV), BF16),
        pltpu.VMEM((2, SHARDS, 32, DV), BF16),
        pltpu.VMEM((2, SHARDS, 32, DV), BF16),
        pltpu.VMEM((2, SHARDS, 32, DV), BF16),
        pltpu.VMEM((2, SHARDS, 32, DV), BF16),
        pltpu.VMEM((LEN, D), BF16),
        pltpu.VMEM((4, LEN, DV), BF16),
        dma((4,)), dma((4,)), dma((WAVES,)), dma((WAVES,)), dma((WAVES, 3)), dma, dma, dma((4,)), dma((4,)),
        dma((WAVES,)), dma((WAVES, 3)), dma((WAVES,)), dma((WAVES, 3)), dma((WAVES,)), dma((WAVES, 3)),
        dma((WAVES,)), dma((WAVES, 3, 2, 2)), dma((WAVES, 3)), dma((WAVES, 3, 2)),
        dma((2,)), dma((2,)), dma((2,)), dma((2,)), dma((4,)), dma((4,)), dma((8,)), dma((8,)),
    ]
    args = (
        tokens, norm_gain[None], w_query, w_key, w_value, w_out, decay_rate[0],
        jnp.asarray(high), jnp.asarray(low),
    )
    return pl.pallas_call(
        kernel,
        out_shape=jax.ShapeDtypeStruct((1, LEN, D), BF16),
        in_specs=[any_spec] * 9,
        out_specs=pl.BlockSpec(memory_space=pltpu.VMEM),
        scratch_shapes=scratch,
        compiler_params=pltpu.CompilerParams(
            collective_id=0, has_side_effects=True, vmem_limit_bytes=44 * 1024 * 1024
        ),
    )(*(pltpu.with_memory_space_constraint(a, pltpu.HBM) for a in args))


def solution(mesh):
    split = Mesh(mesh.devices.reshape(4, 4, 4, 2), ("z", "y", "x", "c"))
    in_specs = (
        P(("x", "c"), ("z", "y"), None),
        P(),
        P(("z", "y", "x", "c"), None),
        P(("z", "y", "x", "c"), None),
        P(("z", "y", "x", "c"), None),
        P(("z", "y", "x", "c"), None),
        P(("x", "c"), None, None),
    )
    return jax.shard_map(
        body, mesh=split, in_specs=in_specs, out_specs=P(("x", "c"), ("z", "y"), None), check_vma=False
    )
```
